32 devices in a mesh: ep: 8 (over z, y), tp: 4 (over x, core).
Axes of the slice: x: 2, y: 2, z: 4, core: 2. Of those that a mesh axis runs over, the one named last changes fastest.
Arguments:
- resid: bfloat16 [256, 2048], P('ep'), may hold values from -6 to 6
- mix_gain: bfloat16 [2048], replicated, may hold values from 0.099609375 to 1.8984375
- proj_x: bfloat16 [2048, 512], P(None, 'tp'), may hold values from -0.125 to 0.125
- proj_z: bfloat16 [2048, 512], P(None, 'tp'), may hold values from -0.125 to 0.125
- proj_b: bfloat16 [2048, 512], P(None, 'tp'), may hold values from -0.125 to 0.125
- proj_c: bfloat16 [2048, 512], P(None, 'tp'), may hold values from -0.125 to 0.125
- proj_step: bfloat16 [2048, 8], replicated, may hold values from -0.125 to 0.125
- step_bias: float32 [8], P('tp'), may hold values from -5 to -1
- decay_rate: float32 [8], P('tp'), may hold values from 1 to 16
- conv_taps: bfloat16 [3, 4, 512], P(None, None, 'tp'), may hold values from -3 to 3
- conv_state: bfloat16 [256, 3, 3, 512], P('ep', None, None, 'tp'), may hold values from -6 to 6
- scan_state: float32 [256, 8, 64, 128], P('ep', 'tp'), may hold values from -2.5 to 2.5
- inner_gain: bfloat16 [512], P('tp'), may hold values from 0.099609375 to 1.8984375
- proj_out: bfloat16 [512, 2048], P('tp'), may hold values from -0.25 to 0.25
- post_gain: bfloat16 [2048], replicated, may hold values from 0.099609375 to 1.8984375
- ffn_gain: bfloat16 [2048], replicated, may hold values from 0.099609375 to 1.8984375
- group_router: bfloat16 [2048, 2], replicated, may hold values from -0.125 to 0.125
- expert_router: bfloat16 [2048, 8], replicated, may hold values from -0.125 to 0.125
- route_experts: int32 [256, 4], P('ep'), may hold values from 0 to 7, as said below
- expert_gate: bfloat16 [8, 2048, 1024], P('ep', None, 'tp'), may hold values from -0.125 to 0.125
- expert_up: bfloat16 [8, 2048, 1024], P('ep', None, 'tp'), may hold values from -0.125 to 0.125
- expert_down: bfloat16 [8, 1024, 2048], P('ep', 'tp')
- dense_switch: bfloat16 [2048], replicated, may hold values from -0.125 to 0.125
- dense_gate: bfloat16 [2048, 2048], P('ep', 'tp'), may hold values from -0.125 to 0.125
- dense_up: bfloat16 [2048, 2048], P('ep', 'tp'), may hold values from -0.125 to 0.125
- dense_down: bfloat16 [2048, 2048], P('ep', 'tp')
- out_gain: bfloat16 [2048], P('tp'), may hold values from 0.099609375 to 1.8984375
Outputs:
- layer_out: bfloat16 [256, 2048], P('ep', 'tp')
- new_state: float32 [256, 8, 64, 128], P('ep', 'tp')
- new_conv: bfloat16 [256, 3, 3, 512], P('ep', None, None, 'tp')
The draws below stay inside these ranges and needn't reach their ends.
Inputs may be any that keep to these rules, and one draw needn't show every extreme that they name: `route_experts`: each row names 4 different experts, all from one group of 4 consecutive expert numbers. Within each aligned block of 32 rows (the rows of one index of ep) no expert is named more than 32 times, and one expert, the same in every block, is named exactly 32 times in every block.
All inputs are finite; a program needn't handle non-finite values.
Results may differ from the reference program's by a relative error of at most 0.019.
Values may be sent and summed in bfloat16 or wider, within the bound.
A program may use at most 64 MiB of HBM per device.

```python
import math
import jax
import jax.numpy as jnp
from jax import lax

MODEL_WIDTH = 2048
HEAD_COUNT = 8
HEAD_DIM = 64
STATE_DIM = 128
STATE_GROUPS = 4
CONV_TAPS = 4
EXPERT_WIDTH = 1024
DENSE_WIDTH = 2048
ROUTE_GROUPS = 2
ROUTE_PICKS = 4
SEQ_DEV = 32
INNER_WIDTH = 512
EXPERTS = 8
GROUP_EXPERTS = 4
CAPACITY = 32
TOKENS = 256
N_TP = 4


def draw_route_experts(key, part):
    blocks = TOKENS // SEQ_DEV
    hot_key, block_key = jax.random.split(jax.random.fold_in(key, 11))
    hot = jax.random.randint(hot_key, (), 0, EXPERTS)
    hot_group = hot // GROUP_EXPERTS
    hot_local = hot % GROUP_EXPERTS
    needed = (CAPACITY - 1) * GROUP_EXPERTS // ROUTE_PICKS + 1

    def one_block(index):
        keys = jax.random.split(jax.random.fold_in(block_key, index), 5)
        hot_rows = jax.random.randint(keys[0], (), needed, SEQ_DEV + 1)
        other = jax.random.randint(keys[1], (SEQ_DEV,), 0, ROUTE_GROUPS - 1)
        other = other + (other >= hot_group).astype(jnp.int32)
        position = jnp.arange(SEQ_DEV)
        group_of = jnp.where(position < hot_rows, hot_group, other)
        group_of = jax.random.permutation(keys[2], group_of)
        member = (group_of[:, None] == jnp.arange(ROUTE_GROUPS)[None, :]).astype(jnp.int32)
        rank = jnp.sum((jnp.cumsum(member, axis=0) - member) * member, axis=1)
        orders = jax.vmap(lambda inner: jax.random.permutation(inner, GROUP_EXPERTS))(jax.random.split(keys[3], ROUTE_GROUPS))
        offsets = jax.random.randint(keys[4], (ROUTE_GROUPS,), 0, GROUP_EXPERTS)
        hot_place = jnp.argmax((orders[hot_group] == hot_local).astype(jnp.int32))
        offsets = offsets.at[hot_group].set(hot_place)
        order_rows = orders[group_of]
        places = (offsets[group_of][:, None] + rank[:, None] * ROUTE_PICKS + jnp.arange(ROUTE_PICKS)[None, :]) % GROUP_EXPERTS
        local = jnp.take_along_axis(order_rows, places, axis=1)
        return (group_of[:, None] * GROUP_EXPERTS + local).astype(jnp.int32)
    return jax.vmap(one_block)(jnp.arange(blocks)).reshape(TOKENS, ROUTE_PICKS)


def column_ramp(width):
    ramp = jnp.arange(width, dtype=jnp.float32) / width
    return 0.5 * jnp.power(10.0, ramp)


def draw_expert_down(key, part):
    base = jax.random.truncated_normal(jax.random.fold_in(key, 21), -6.0, 6.0, (EXPERTS, EXPERT_WIDTH, MODEL_WIDTH), jnp.float32)
    base = base * EXPERT_WIDTH ** (-0.5)
    return (base * column_ramp(MODEL_WIDTH)[None, None, :]).astype(jnp.bfloat16)


def draw_dense_down(key, part):
    base = jax.random.truncated_normal(jax.random.fold_in(key, 31), -6.0, 6.0, (DENSE_WIDTH, MODEL_WIDTH), jnp.float32)
    base = base * DENSE_WIDTH ** (-0.5)
    return (base * column_ramp(MODEL_WIDTH)[None, :]).astype(jnp.bfloat16)


def shard_levels(own_key, shape, shards, smallest, top_value):
    level, own = 1.0, jax.random.fold_in(own_key, 6)
    for dim, blocks in shards:
        heights = jnp.exp(jax.random.uniform(jax.random.fold_in(own, dim), (blocks,), jnp.float32, smallest / len(shards), top_value / len(shards)))
        level = level * jnp.repeat(heights, shape[dim] // blocks).reshape([-1 if axis == dim else 1 for axis in range(len(shape))])
    return level


def normal_values(stream_key, extent, scale, limit, shards=(), held_as=jnp.bfloat16):
    values = jax.random.normal(stream_key, extent, jnp.float32) * scale
    if len(shards) > 0:
        values = shard_levels(stream_key, extent, shards, -0.22, 0.18) * values
    return jnp.clip(values, min=-limit, max=limit).astype(held_as)


def setup_inputs(seed: int = 0) -> dict:
    key_of = jax.random.split(jax.random.key(seed), 28)
    resid = normal_values(key_of[0], (TOKENS, MODEL_WIDTH), 1.0, 6.0, ((0, 8),))
    mix_gain = jnp.clip(1.0 + 0.18 * jax.random.normal(key_of[1], (MODEL_WIDTH,), jnp.float32), 0.099609375, 1.8984375).astype(jnp.bfloat16)
    proj_x = normal_values(key_of[2], (MODEL_WIDTH, INNER_WIDTH), MODEL_WIDTH ** -0.5, 0.125, ((1, 4),))
    proj_z = normal_values(key_of[3], (MODEL_WIDTH, INNER_WIDTH), MODEL_WIDTH ** -0.5, 0.125, ((1, 4),))
    proj_b = normal_values(key_of[4], (MODEL_WIDTH, STATE_GROUPS * STATE_DIM), MODEL_WIDTH ** -0.5, 0.125, ((1, 4),))
    proj_c = normal_values(key_of[5], (MODEL_WIDTH, STATE_GROUPS * STATE_DIM), MODEL_WIDTH ** -0.5, 0.125, ((1, 4),))
    proj_step = normal_values(key_of[6], (MODEL_WIDTH, HEAD_COUNT), MODEL_WIDTH ** -0.5, 0.125)
    step_bias = jnp.clip(-5.0 + 4.0 * jax.random.uniform(key_of[7], (HEAD_COUNT,), jnp.float32) ** shard_levels(key_of[7], (HEAD_COUNT,), ((0, 4),), -0.2, 0.2), -5.0, -1.0)
    decay_rate = jnp.clip(jnp.exp(math.log(16.0) - 2.7725887 * jax.random.uniform(key_of[8], (HEAD_COUNT,), jnp.float32) ** shard_levels(key_of[8], (HEAD_COUNT,), ((0, 4),), -0.2, 0.2)), 1.0, 16.0)
    conv_taps = normal_values(key_of[9], (3, CONV_TAPS, INNER_WIDTH), CONV_TAPS ** -0.5, 3.0, ((2, 4),))
    conv_state = normal_values(key_of[10], (TOKENS, 3, CONV_TAPS - 1, INNER_WIDTH), 1.0, 6.0, ((0, 8), (3, 4)))
    scan_state = normal_values(key_of[11], (TOKENS, HEAD_COUNT, HEAD_DIM, STATE_DIM), 0.3, 2.5, ((0, 8), (1, 4)), jnp.float32)
    inner_gain = jnp.clip(1.0 + 0.18 * jax.random.normal(key_of[12], (INNER_WIDTH,), jnp.float32), 0.099609375, 1.8984375).astype(jnp.bfloat16)
    proj_out = normal_values(key_of[13], (INNER_WIDTH, MODEL_WIDTH), INNER_WIDTH ** -0.5, 0.25, ((0, 4),))
    post_gain = jnp.clip(1.0 + 0.18 * jax.random.normal(key_of[14], (MODEL_WIDTH,), jnp.float32), 0.099609375, 1.8984375).astype(jnp.bfloat16)
    ffn_gain = jnp.clip(1.0 + 0.18 * jax.random.normal(key_of[15], (MODEL_WIDTH,), jnp.float32), 0.099609375, 1.8984375).astype(jnp.bfloat16)
    group_router = normal_values(key_of[16], (MODEL_WIDTH, ROUTE_GROUPS), MODEL_WIDTH ** -0.5, 0.125)
    expert_router = normal_values(key_of[17], (MODEL_WIDTH, EXPERTS), MODEL_WIDTH ** -0.5, 0.125)
    route_experts = draw_route_experts(jax.random.fold_in(key_of[27], 71), 0)
    expert_gate = normal_values(key_of[19], (EXPERTS, MODEL_WIDTH, EXPERT_WIDTH), MODEL_WIDTH ** -0.5, 0.125, ((0, 8), (2, 4)))
    expert_up = normal_values(key_of[20], (EXPERTS, MODEL_WIDTH, EXPERT_WIDTH), MODEL_WIDTH ** -0.5, 0.125, ((0, 8), (2, 4)))
    expert_down = draw_expert_down(jax.random.fold_in(key_of[27], 71), 0)
    dense_switch = normal_values(key_of[22], (MODEL_WIDTH,), MODEL_WIDTH ** -0.5, 0.125)
    dense_gate = normal_values(key_of[23], (DENSE_WIDTH, MODEL_WIDTH), MODEL_WIDTH ** -0.5, 0.125, ((0, 8), (1, 4)))
    dense_up = normal_values(key_of[24], (DENSE_WIDTH, MODEL_WIDTH), MODEL_WIDTH ** -0.5, 0.125, ((0, 8), (1, 4)))
    dense_down = draw_dense_down(jax.random.fold_in(key_of[27], 71), 0)
    out_gain = jnp.clip(1.0 + 0.18 * jax.random.normal(key_of[26], (MODEL_WIDTH,), jnp.float32), 0.099609375, 1.8984375).astype(jnp.bfloat16)
    return dict(resid=resid, mix_gain=mix_gain, proj_x=proj_x, proj_z=proj_z, proj_b=proj_b, proj_c=proj_c, proj_step=proj_step, step_bias=step_bias, decay_rate=decay_rate, conv_taps=conv_taps, conv_state=conv_state, scan_state=scan_state, inner_gain=inner_gain, proj_out=proj_out, post_gain=post_gain, ffn_gain=ffn_gain, group_router=group_router, expert_router=expert_router, route_experts=route_experts, expert_gate=expert_gate, expert_up=expert_up, expert_down=expert_down, dense_switch=dense_switch, dense_gate=dense_gate, dense_up=dense_up, dense_down=dense_down, out_gain=out_gain)


norm_eps = 1e-06

def scaled_rows(values, gain):
    values = values.astype(jnp.float32)
    mean_square = lax.optimization_barrier(jnp.mean(values * values, axis=-1, keepdims=True))
    return values * lax.rsqrt(mean_square + norm_eps) * gain.astype(jnp.float32)

def softmax_plain(logits):
    weights = jnp.exp(logits)
    return weights / lax.optimization_barrier(jnp.sum(weights, axis=-1, keepdims=True))

def state_block(pieces):
    old_state, keep, driven, b_heads, c_heads = pieces
    updated = keep[:, :, None, None] * old_state + driven[:, :, :, None] * b_heads[:, :, None, :]
    read = lax.optimization_barrier(jnp.sum(updated * c_heads[:, :, None, :], axis=3))
    return (updated, read)

def expert_block(pieces):
    rows, gate_weight, up_weight, down_weight = pieces
    gate_value = jnp.dot(rows, gate_weight, preferred_element_type=jnp.float32)
    up_value = jnp.dot(rows, up_weight, preferred_element_type=jnp.float32)
    hidden = (jax.nn.silu(gate_value) * up_value).astype(jnp.bfloat16)
    share = hidden.shape[1] // N_TP
    parts = jnp.einsum('rqf,qfd->qrd', hidden.reshape(rows.shape[0], N_TP, share).astype(jnp.float32), down_weight.reshape(N_TP, share, down_weight.shape[1]).astype(jnp.float32))
    parts = lax.optimization_barrier(parts.astype(jnp.bfloat16))
    return lax.optimization_barrier(jnp.sum(parts.astype(jnp.float32), axis=0)).astype(jnp.bfloat16)

def reference(resid, mix_gain, proj_x, proj_z, proj_b, proj_c, proj_step, step_bias, decay_rate, conv_taps, conv_state, scan_state, inner_gain, proj_out, post_gain, ffn_gain, group_router, expert_router, route_experts, expert_gate, expert_up, expert_down, dense_switch, dense_gate, dense_up, dense_down, out_gain):
    normed = scaled_rows(resid, mix_gain).astype(jnp.bfloat16)
    fresh = jnp.stack([jnp.dot(normed, proj_x, preferred_element_type=jnp.float32), jnp.dot(normed, proj_b, preferred_element_type=jnp.float32), jnp.dot(normed, proj_c, preferred_element_type=jnp.float32)], axis=1).astype(jnp.bfloat16)
    gate_z = jnp.dot(normed, proj_z, preferred_element_type=jnp.float32)
    step_raw = jnp.dot(normed, proj_step, preferred_element_type=jnp.float32)
    history = jnp.concatenate([conv_state, fresh[:, :, None, :]], axis=2)
    activated = jax.nn.silu(lax.optimization_barrier(jnp.sum(history.astype(jnp.float32) * conv_taps.astype(jnp.float32)[None], axis=2)))
    repeat = HEAD_COUNT // STATE_GROUPS
    xs_heads = activated[:, 0].reshape(TOKENS, HEAD_COUNT, HEAD_DIM)
    b_heads = jnp.repeat(activated[:, 1].reshape(TOKENS, STATE_GROUPS, STATE_DIM), repeat, axis=1)
    c_heads = jnp.repeat(activated[:, 2].reshape(TOKENS, STATE_GROUPS, STATE_DIM), repeat, axis=1)
    step = jax.nn.softplus(step_raw + step_bias)
    keep = jnp.exp(-decay_rate * step)
    driven = step[:, :, None] * xs_heads
    blocks = TOKENS // SEQ_DEV

    def by_block(array):
        return array.reshape((blocks, SEQ_DEV) + array.shape[1:])
    new_state, read = lax.map(state_block, (by_block(scan_state), by_block(keep), by_block(driven), by_block(b_heads), by_block(c_heads)))
    new_state = new_state.reshape(scan_state.shape)
    read = read.reshape(TOKENS, INNER_WIDTH)
    gated = (read * jax.nn.silu(gate_z) * inner_gain.astype(jnp.float32)).astype(jnp.bfloat16)
    mixed = jnp.dot(gated, proj_out, preferred_element_type=jnp.float32)
    stream = (resid.astype(jnp.float32) + scaled_rows(mixed, post_gain)).astype(jnp.bfloat16)
    feed = scaled_rows(stream, ffn_gain).astype(jnp.bfloat16)
    group_prob = softmax_plain(jnp.dot(feed, group_router, preferred_element_type=jnp.float32))
    expert_logits = jnp.dot(feed, expert_router, preferred_element_type=jnp.float32)
    matches = route_experts[:, :, None] == jnp.arange(EXPERTS, dtype=jnp.int32)[None, None, :]
    pick_logits = lax.optimization_barrier(jnp.sum(jnp.where(matches, expert_logits[:, None, :], 0.0), axis=2))
    chosen_group = route_experts[:, 0] // GROUP_EXPERTS
    group_weight = lax.optimization_barrier(jnp.sum(jnp.where(chosen_group[:, None] == jnp.arange(ROUTE_GROUPS, dtype=jnp.int32)[None, :], group_prob, 0.0), axis=1))
    pick_weight = softmax_plain(pick_logits) * group_weight[:, None]
    flat_picks = route_experts.reshape(blocks, SEQ_DEV * ROUTE_PICKS)
    one_hot = (flat_picks[:, :, None] == jnp.arange(EXPERTS, dtype=jnp.int32)[None, None, :]).astype(jnp.int32)
    slot = lax.optimization_barrier(jnp.sum((jnp.cumsum(one_hot, axis=1) - one_hot) * one_hot, axis=2))
    block_ids = jnp.arange(blocks, dtype=jnp.int32)[:, None]
    target = ((flat_picks * blocks + block_ids) * CAPACITY + slot).reshape(-1).astype(jnp.int32)
    repeated = jnp.repeat(feed, ROUTE_PICKS, axis=0)
    buffer = jnp.zeros((EXPERTS * blocks * CAPACITY, MODEL_WIDTH), jnp.bfloat16).at[target].set(repeated)
    served = lax.map(expert_block, (buffer.reshape(EXPERTS, blocks * CAPACITY, MODEL_WIDTH), expert_gate, expert_up, expert_down))
    expert_out = served.reshape(-1, MODEL_WIDTH)[target].reshape(TOKENS, ROUTE_PICKS, MODEL_WIDTH)
    routed = lax.optimization_barrier(jnp.sum(expert_out.astype(jnp.float32) * pick_weight[:, :, None], axis=1))
    dense_pre_gate = jnp.dot(feed, dense_gate.T, preferred_element_type=jnp.float32)
    dense_pre_up = jnp.dot(feed, dense_up.T, preferred_element_type=jnp.float32)
    dense_hidden = (jax.nn.silu(dense_pre_gate) * dense_pre_up).astype(jnp.bfloat16)
    dense_out = jnp.dot(dense_hidden, dense_down, preferred_element_type=jnp.float32)
    switch = jax.nn.sigmoid(jnp.dot(feed, dense_switch, preferred_element_type=jnp.float32))
    combined = routed + switch[:, None] * dense_out
    layer_out = (stream.astype(jnp.float32) + scaled_rows(combined, out_gain)).astype(jnp.bfloat16)
    new_conv = history[:, :, 1:, :]
    return (layer_out, new_state, new_conv)
```

```python
import functools

import jax
import jax.numpy as jnp
from jax import lax
from jax.experimental import pallas as pl
from jax.experimental.pallas import tpu as pltpu
from jax.sharding import PartitionSpec as P

norm_eps = 1e-06


def scaled_rows(values, gain):
    values = values.astype(jnp.float32)
    mean_square = jnp.mean(values * values, axis=-1, keepdims=True)
    return values * lax.rsqrt(mean_square + norm_eps) * gain.astype(jnp.float32)


def softmax_plain(logits):
    weights = jnp.exp(logits)
    return weights / jnp.sum(weights, axis=-1, keepdims=True)


def fused_kernel(
    ep,
    group_size,
    group_count,
    expert_count,
    proj_out_ref,
    resid_ref,
    mix_ref,
    post_ref,
    ffn_ref,
    expert_router_ref,
    group_router_ref,
    switch_ref,
    route_ref,
    out_gain_ref,
    inner_ref,
    proj_step_ref,
    taps_ref,
    conv_ref,
    bias_ref,
    decay_ref,
    proj_x_hbm,
    proj_z_hbm,
    proj_b_hbm,
    proj_c_hbm,
    state_hbm,
    gate_hbm,
    up_hbm,
    down_hbm,
    dense_gate_hbm,
    dense_up_hbm,
    dense_down_hbm,
    out_ref,
    new_state_hbm,
    new_conv_ref,
    proj_w,
    state_buf,
    new_state_buf,
    router_buf,
    gate_w,
    up_w,
    down_w,
    dgate,
    dup,
    ddown,
    stream_buf,
    mix_own,
    mix_peer,
    half_own,
    half_far,
    rows_buf,
    aux_buf,
    part_buf,
    part_peer,
    send_x,
    recv_x,
    send_ep,
    recv_ep,
    square_own,
    square_peer,
    local_sem,
    state_sem,
    dense_send,
    dense_recv,
    mix_send,
    mix_recv,
    rows_send,
    rows_recv,
    aux_send,
    aux_recv,
    part_send,
    part_recv,
    x_send,
    x_recv,
    ep_send,
    ep_recv,
    square_send,
    square_recv,
    entered,
    z_send,
    z_aux_send,
):
    f32, bf16 = jnp.float32, jnp.bfloat16
    me = lax.axis_index("ep")
    tp = lax.axis_index("tp")
    far = tp // 2
    core = tp % 2
    beside = far * 2 + (1 - core)
    across = (1 - far) * 2 + core
    diagonal = (1 - far) * 2 + (1 - core)
    near = (beside, across, diagonal)
    seqs, width = resid_ref.shape
    quarter = width // 4
    share = dgate.shape[1]

    def remote(src, dst, send, recv, ep_to, tp_to):
        return pltpu.make_async_remote_copy(
            src_ref=src,
            dst_ref=dst,
            send_sem=send,
            recv_sem=recv,
            device_id=(ep_to, tp_to),
            device_id_type=pl.DeviceIdType.MESH,
        )

    def ep_at(step):
        return lax.rem(me + step + ep, ep)

    local = []

    def load(src, dst):
        copy = pltpu.make_async_copy(src, dst, local_sem.at[len(local)])
        copy.start()
        local.append(copy)

    for k, src in enumerate((proj_x_hbm, proj_b_hbm, proj_c_hbm, proj_z_hbm)):
        load(src, proj_w.at[k])
    load(state_hbm, state_buf)
    load(gate_hbm.at[0], gate_w)
    load(up_hbm.at[0], up_w)
    for q in range(4):
        load(down_hbm.at[0, :, pl.ds(q * quarter, quarter)], down_w.at[q])
    dense_pairs = ((dense_gate_hbm, dgate), (dense_up_hbm, dup), (dense_down_hbm, ddown))
    for src, dst in dense_pairs:
        load(src.at[pl.ds(tp * share, share), :], dst.at[tp])

    barrier = pltpu.get_barrier_semaphore()
    for step in range(1, ep):

        @pl.when(me + step < ep)
        def _():
            pl.semaphore_signal(
                barrier, inc=1, device_id=(ep_at(step), tp), device_id_type=pl.DeviceIdType.MESH
            )

    for peer in near:
        pl.semaphore_signal(
            barrier, inc=1, device_id=(me, peer), device_id_type=pl.DeviceIdType.MESH
        )

    def row(ref):
        return ref[...].astype(f32).reshape(1, ref.shape[0])

    resid_f = resid_ref[...].astype(f32)
    resid_scale = lax.rsqrt(jnp.mean(resid_f * resid_f, axis=1, keepdims=True) + norm_eps)
    normed = (resid_f * resid_scale * row(mix_ref)).astype(bf16)
    group_base = -(-expert_count // 8) * 8
    switch_lane = group_base + -(-group_count // 8) * 8
    router_buf[...] = jnp.zeros_like(router_buf)
    router_buf[0:expert_count, :] = expert_router_ref[...].astype(f32)
    router_buf[group_base : group_base + group_count, :] = group_router_ref[...].astype(f32)
    router_buf[switch_lane : switch_lane + 1, :] = row(switch_ref)
    nt = (((1,), (1,)), ((), ()))
    step_all = lax.dot_general(normed, proj_step_ref[...], nt, preferred_element_type=f32)
    pl.semaphore_wait(barrier, me + 3)
    for step in range(1, ep):

        @pl.when(me >= step)
        def _():
            pl.semaphore_signal(
                entered, inc=1, device_id=(me - step, tp), device_id_type=pl.DeviceIdType.MESH
            )


    sends = []
    dense_copies = []

    def send_dense(t):
        src, dst = dense_pairs[t]
        for k, peer in enumerate(near):
            copy = remote(
                src.at[pl.ds(peer * share, share), :],
                dst.at[tp],
                dense_send.at[3 * t + k],
                dense_recv.at[3 * t + k],
                me,
                peer,
            )
            copy.start()
            dense_copies.append(copy)

    send_dense(0)
    send_dense(1)

    channels = conv_ref.shape[3]
    heads = bias_ref.shape[0]
    head_dim = channels // heads
    taps = taps_ref[...].astype(f32)
    old = conv_ref.shape[1]
    active = []
    for k in range(3):
        local[k].wait()
        fresh = jnp.dot(normed, proj_w[k], preferred_element_type=f32).astype(bf16)
        summed = conv_ref[k, 0].astype(f32) * taps[k, 0:1]
        for tap in range(1, old):
            earlier = conv_ref[k, tap]
            new_conv_ref[k, tap - 1] = earlier
            summed = summed + earlier.astype(f32) * taps[k, tap : tap + 1]
        new_conv_ref[k, old - 1] = fresh
        summed = summed + fresh.astype(f32) * taps[k, old : old + 1]
        active.append(summed * jax.nn.sigmoid(summed))
    inputs, vec_in, vec_read = active
    local[3].wait()
    gate_z = jnp.dot(normed, proj_w[3], preferred_element_type=f32)
    step_lane = lax.broadcasted_iota(jnp.int32, step_all.shape, 1)
    lane_in = lax.broadcasted_iota(jnp.int32, (seqs, channels), 1)
    keep = jnp.zeros((seqs, channels), f32)
    stepped = jnp.zeros((seqs, channels), f32)
    for h in range(heads):
        raw = jnp.sum(
            jnp.where(step_lane == tp * heads + h, step_all, 0.0), axis=1, keepdims=True
        )
        raw = raw + bias_ref[h]
        step = jnp.maximum(raw, 0.0) + jnp.log1p(jnp.exp(-jnp.abs(raw)))
        mine = (lane_in >= h * head_dim) & (lane_in < (h + 1) * head_dim)
        keep = jnp.where(mine, jnp.exp(-decay_ref[h] * step), keep)
        stepped = jnp.where(mine, step, stepped)
    columns = jnp.concatenate(
        [keep, stepped * inputs, jnp.zeros((channels - 2 * seqs, channels), f32)], axis=0
    ).T
    local[4].wait()
    read_lane = lax.broadcasted_iota(jnp.int32, (channels, channels), 1)
    read = jnp.zeros((channels, channels), f32)
    for t in range(seqs):
        fresh_state = (
            columns[:, t : t + 1] * state_buf[t]
            + columns[:, seqs + t : seqs + t + 1] * vec_in[t : t + 1]
        )
        new_state_buf[t] = fresh_state
        value = jnp.sum(fresh_state * vec_read[t : t + 1], axis=1, keepdims=True)
        read = jnp.where(read_lane == t, value, read)
    read = read.T[0:seqs]
    gated = (read * (gate_z * jax.nn.sigmoid(gate_z)) * row(inner_ref)).astype(bf16)
    mix_own[...] = jnp.dot(gated, proj_out_ref[...], preferred_element_type=f32).astype(bf16)

    first = remote(mix_own, mix_peer, mix_send.at[0], mix_recv.at[0], me, beside)
    first.start()
    sends.append(first)
    first.wait_recv()
    half = width // 2
    chip_sum = (mix_own[...].astype(f32) + mix_peer[...].astype(f32)).astype(bf16)
    half_own[0] = chip_sum[:, :half]
    half_own[1] = chip_sum[:, half:]
    over_x = remote(
        half_own.at[core], half_far.at[core], mix_send.at[1], mix_recv.at[1], me, across
    )
    over_x.start()
    send_dense(2)
    sends += dense_copies

    state_out = pltpu.make_async_copy(new_state_buf, new_state_hbm, state_sem)
    state_out.start()
    over_x.wait_recv()
    to_core = remote(
        half_far.at[core], half_far.at[core], mix_send.at[2], mix_recv.at[2], me, beside
    )
    to_core.start()
    sends += [over_x, to_core]
    to_core.wait_recv()

    far_sum = jnp.concatenate([half_far[0], half_far[1]], axis=1)
    mixed = chip_sum.astype(f32) + far_sum.astype(f32)
    mixed_scale = lax.rsqrt(jnp.mean(mixed * mixed, axis=1, keepdims=True) + norm_eps)
    stream = (
        resid_f + mixed * mixed_scale * row(post_ref)
    ).astype(bf16)
    stream_f = stream.astype(f32)
    feed_scale = lax.rsqrt(jnp.mean(stream_f * stream_f, axis=1, keepdims=True) + norm_eps)
    feed_f = stream_f * feed_scale * row(ffn_ref)
    feed = feed_f.astype(bf16)
    my_z, my_y = me // 2, me % 2
    nz = ep // 2
    here = my_y * nz + my_z

    def feed_of(q):
        value = feed_f[:, :quarter]
        for other in range(1, 4):
            piece = feed_f[:, other * quarter : (other + 1) * quarter]
            value = jnp.where(q == other, piece, value)
        return value.astype(bf16)

    quarters = (tp, beside, across, diagonal)
    for k, q in enumerate(quarters):
        rows_buf[k, here] = feed_of(q)
    for q in range(4):
        stream_buf[q] = stream[:, q * quarter : (q + 1) * quarter]

    @pl.when(me + 1 < ep)
    def _():
        pl.semaphore_wait(entered, ep - 1 - me)

    others = [j + (j - my_z + nz) // nz for j in range(nz - 1)]

    def rows_copy(k, at, send, ep_to, tp_to, k_to):
        return remote(
            rows_buf.at[k, at],
            rows_buf.at[k_to, at],
            rows_send.at[send, at],
            rows_recv.at[k_to, at],
            ep_to,
            tp_to,
        )

    def aux_copy(at, send, ep_to):
        return remote(
            aux_buf.at[at], aux_buf.at[at], aux_send.at[send, at], aux_recv.at[at], ep_to, tp
        )

    def z_rows(z):
        return remote(
            rows_buf.at[0, here],
            rows_buf.at[0, here],
            z_send.at[z],
            rows_recv.at[0, here],
            z * 2 + my_y,
            tp,
        )

    def z_aux(z):
        return remote(
            aux_buf.at[here], aux_buf.at[here], z_aux_send.at[z], aux_recv.at[here],
            z * 2 + my_y, tp,
        )

    def started(copy):
        copy.start()
        sends.append(copy)

    for z in reversed(others):
        started(z_rows(z))
    over_y = my_z * 2 + 1 - my_y
    started(rows_copy(0, here, 0, over_y, tp, 0))
    started(rows_copy(2, here, 1, over_y, tp, 2))

    logits = lax.dot_general(
        feed, router_buf[...].astype(bf16), nt, preferred_element_type=f32
    )
    lane = lax.broadcasted_iota(jnp.int32, logits.shape, 1)
    same = lax.broadcasted_iota(jnp.int32, (seqs, seqs), 0) == lax.broadcasted_iota(
        jnp.int32, (seqs, seqs), 1
    )
    route = lax.dot_general(
        jnp.where(same, 1.0, 0.0).astype(bf16),
        route_ref[...].astype(f32).astype(bf16),
        nt,
        preferred_element_type=f32,
    ).astype(jnp.int32)
    picked = lane == route[:, 0:1]
    for k in range(1, route.shape[1]):
        picked = picked | (lane == route[:, k : k + 1])
    weights = jnp.exp(logits)
    pick = jnp.where(picked, weights, 0.0)
    group_lane = (lane - group_base) * group_size
    in_groups = (lane >= group_base) & (lane < group_base + group_count)
    group = jnp.where(in_groups, weights, 0.0)
    lead = route[:, 0:1]
    chosen = in_groups & (lead >= group_lane) & (lead < group_lane + group_size)
    group_weight = jnp.sum(jnp.where(chosen, weights, 0.0), axis=1, keepdims=True) / jnp.sum(
        group, axis=1, keepdims=True
    )
    pick = pick / jnp.sum(pick, axis=1, keepdims=True) * group_weight
    aux_buf[here] = jnp.where(lane == switch_lane, jax.nn.sigmoid(logits), pick).astype(bf16)
    for z in reversed(others):
        started(z_aux(z))
    started(aux_copy(here, 0, over_y))

    total = nz * seqs
    sides = (my_y, 1 - my_y)

    def at_of(side, z):
        return sides[side] * nz + z

    def arrived(k, at):
        rows_copy(k, at, 0, me, beside, k).wait_recv()

    there = at_of(1, my_z)
    for z in others:
        at = at_of(0, z)
        arrived(0, at)
        started(rows_copy(0, at, 0, over_y, tp, 0))
        started(rows_copy(0, at, 1, me, across, 2))
        started(rows_copy(0, at, 2, me, beside, 1))
    arrived(0, there)
    started(rows_copy(0, there, 2, me, beside, 1))
    arrived(2, there)
    started(rows_copy(2, there, 3, me, beside, 3))
    for z in others:
        at = at_of(0, z)
        aux_copy(at, 0, me).wait_recv()
        started(aux_copy(at, 0, over_y))
    for z in others:
        at = at_of(1, z)
        arrived(0, at)
        started(rows_copy(0, at, 1, me, across, 2))
        started(rows_copy(0, at, 2, me, beside, 1))
    for z in others:
        at = at_of(0, z)
        arrived(2, at)
        started(rows_copy(2, at, 3, me, beside, 3))

    def gather_end(side):
        for z in range(nz) if side else others:
            at = at_of(side, z)
            if side:
                aux_copy(at, 0, me).wait_recv()
            arrived(1, at)
            arrived(3, at)

    def add(total_sum, value):
        return value if total_sum is None else total_sum + value

    def part_copy(k, side):
        block = pl.ds(sides[side] * nz, nz)
        return remote(
            part_buf.at[(diagonal, beside)[k], block],
            part_peer.at[k, block],
            part_send.at[k, side],
            part_recv.at[k, side],
            me,
            beside,
        )

    def feed_forward(side):
        block = pl.ds(sides[side] * nz, nz)
        gate = up = dense_g = dense_u = None
        for k, q in enumerate(quarters):
            rows = rows_buf[k, block].reshape(total, quarter)
            span = pl.ds(pl.multiple_of(q * quarter, quarter), quarter)
            gate = add(gate, jnp.dot(rows, gate_w[span, :], preferred_element_type=f32))
            up = add(up, jnp.dot(rows, up_w[span, :], preferred_element_type=f32))
            dense_g = add(
                dense_g, lax.dot_general(rows, dgate[q], nt, preferred_element_type=f32)
            )
            dense_u = add(dense_u, lax.dot_general(rows, dup[q], nt, preferred_element_type=f32))
        aux = aux_buf[block].reshape(total, aux_buf.shape[2]).astype(f32)
        aux_lane = lax.broadcasted_iota(jnp.int32, aux.shape, 1)
        weight = jnp.sum(jnp.where(aux_lane == me, aux, 0.0), axis=1, keepdims=True)
        switch = jnp.sum(jnp.where(aux_lane == switch_lane, aux, 0.0), axis=1, keepdims=True)
        hidden = (gate * jax.nn.sigmoid(gate) * up * weight).astype(bf16)
        dense_hidden = (dense_g * jax.nn.sigmoid(dense_g) * dense_u * switch).astype(bf16)
        for k, q in enumerate((diagonal, beside, across, tp)):
            value = jnp.dot(hidden, down_w[q], preferred_element_type=f32) + jnp.dot(
                dense_hidden, ddown[q], preferred_element_type=f32
            )
            part_buf[q, block] = value.astype(bf16).reshape(nz, seqs, quarter)
            if k < 2:
                started(part_copy(k, side))

    def targets(side):
        return list(range(nz)) if side else others + [my_z]

    def x_copy(at):
        return remote(send_x.at[at], recv_x.at[at], x_send.at[at], x_recv.at[at], me, across)

    def sums_over_x(side):
        part_copy(0, side).wait_recv()
        for z in targets(side):
            at = at_of(side, z)
            send_x[at] = (
                part_buf[across, at].astype(f32) + part_peer[0, at].astype(f32)
            ).astype(bf16)
            started(x_copy(at))

    def ep_copy(at, slot, ep_to):
        return remote(
            send_ep.at[at], recv_ep.at[slot], ep_send.at[at], ep_recv.at[slot], ep_to, tp
        )

    def summed(at):
        x_copy(at).wait_recv()
        return (
            part_buf[tp, at].astype(f32)
            + part_peer[1, at].astype(f32)
            + recv_x[at].astype(f32)
        )

    def sums_over_ep(side):
        part_copy(1, side).wait_recv()
        for z in range(nz) if side else others:
            at = at_of(side, z)
            send_ep[at] = summed(at).astype(bf16)
            started(ep_copy(at, here, z * 2 + sides[side]))

    for copy in local[5:]:
        copy.wait()
    for copy in dense_copies:
        copy.wait_recv()
    gather_end(0)
    feed_forward(0)
    for z in others:
        at = at_of(1, z)
        arrived(2, at)
        started(rows_copy(2, at, 3, me, beside, 3))
    sums_over_x(0)
    gather_end(1)
    feed_forward(1)
    sums_over_ep(0)
    sums_over_x(1)
    combined = summed(here)
    sums_over_ep(1)

    for side in range(2):
        for z in range(nz) if side else others:
            at = at_of(side, z)
            ep_copy(at, at, me).wait_recv()
            combined = combined + recv_ep[at].astype(f32)

    square = jnp.sum(combined * combined, axis=1, keepdims=True)
    square_own[...] = jnp.broadcast_to(square, square_own.shape)
    square_copies = []
    for k, peer in enumerate(near):
        copy = remote(
            square_own, square_peer.at[k], square_send.at[k], square_recv.at[k], me, peer
        )
        copy.start()
        square_copies.append(copy)
    sends += square_copies
    for copy in square_copies:
        copy.wait_recv()
    everything = (square_own[...] + square_peer[0]) + (square_peer[1] + square_peer[2])
    scale = lax.rsqrt(everything[:, 0:1] / width + norm_eps)
    own_stream = stream_buf[tp].astype(f32)
    out_ref[...] = (own_stream + combined * scale * row(out_gain_ref)).astype(bf16)
    state_out.wait()
    for copy in sends:
        copy.wait_send()


def fused_layer(
    resid,
    mix_gain,
    proj_x,
    proj_z,
    proj_b,
    proj_c,
    proj_step,
    step_bias,
    decay_rate,
    conv_taps,
    conv_state,
    scan_state,
    inner_gain,
    proj_out,
    post_gain,
    ffn_gain,
    group_router,
    expert_router,
    route_experts,
    expert_gate,
    expert_up,
    expert_down,
    dense_switch,
    dense_gate,
    dense_up,
    dense_down,
    out_gain,
):
    ep = lax.axis_size("ep")
    seqs, width = resid.shape
    quarter = width // 4
    channels = conv_state.shape[3]
    expert_count = expert_router.shape[1]
    group_count = group_router.shape[1]
    lanes = 128
    hidden_here = expert_gate.shape[2]
    share = dense_gate.shape[0] // 4
    bf16 = jnp.bfloat16
    vmem = pl.BlockSpec(memory_space=pltpu.VMEM)
    hbm = pl.BlockSpec(memory_space=pl.ANY)
    dma = pltpu.SemaphoreType.DMA
    kernel = functools.partial(
        fused_kernel, ep, expert_count // group_count, group_count, expert_count
    )
    smem = pl.BlockSpec(memory_space=pltpu.SMEM)
    earlier = conv_state.transpose(1, 2, 0, 3)
    state = scan_state.reshape(seqs, channels, scan_state.shape[3])
    layer_out, new_state, new_conv = pl.pallas_call(
        kernel,
        out_shape=(
            jax.ShapeDtypeStruct((seqs, quarter), bf16),
            jax.ShapeDtypeStruct(state.shape, state.dtype),
            jax.ShapeDtypeStruct(earlier.shape, earlier.dtype),
        ),
        in_specs=[vmem] * 14 + [smem] * 2 + [hbm] * 11,
        out_specs=(vmem, hbm, vmem),
        scratch_shapes=[
            pltpu.VMEM((4,) + proj_x.shape, bf16),
            pltpu.VMEM(state.shape, state.dtype),
            pltpu.VMEM(state.shape, state.dtype),
            pltpu.VMEM((lanes, width), jnp.float32),
            pltpu.VMEM((width, hidden_here), bf16),
            pltpu.VMEM((width, hidden_here), bf16),
            pltpu.VMEM((4, hidden_here, quarter), bf16),
            pltpu.VMEM((4, share, quarter), bf16),
            pltpu.VMEM((4, share, quarter), bf16),
            pltpu.VMEM((4, share, quarter), bf16),
            pltpu.VMEM((4, seqs, quarter), bf16),
            pltpu.VMEM((seqs, width), bf16),
            pltpu.VMEM((seqs, width), bf16),
            pltpu.VMEM((2, seqs, width // 2), bf16),
            pltpu.VMEM((2, seqs, width // 2), bf16),
            pltpu.VMEM((4, ep, seqs, quarter), bf16),
            pltpu.VMEM((ep, seqs, lanes), bf16),
            pltpu.VMEM((4, ep, seqs, quarter), bf16),
            pltpu.VMEM((2, ep, seqs, quarter), bf16),
            pltpu.VMEM((ep, seqs, quarter), bf16),
            pltpu.VMEM((ep, seqs, quarter), bf16),
            pltpu.VMEM((ep, seqs, quarter), bf16),
            pltpu.VMEM((ep, seqs, quarter), bf16),
            pltpu.VMEM((seqs, 128), jnp.float32),
            pltpu.VMEM((3, seqs, 128), jnp.float32),
            dma((14,)),
            dma,
            dma((9,)),
            dma((9,)),
            dma((3,)),
            dma((3,)),
            dma((4, ep)),
            dma((4, ep)),
            dma((1, ep)),
            dma((ep,)),
            dma((2, 2)),
            dma((2, 2)),
            dma((ep,)),
            dma((ep,)),
            dma((ep,)),
            dma((ep,)),
            dma((3,)),
            dma((3,)),
            pltpu.SemaphoreType.REGULAR,
            dma((ep,)),
            dma((ep,)),
        ],
        compiler_params=pltpu.CompilerParams(collective_id=0, has_side_effects=True),
        name="fused_layer",
    )(
        proj_out,
        resid,
        mix_gain,
        post_gain,
        ffn_gain,
        expert_router.T,
        group_router.T,
        dense_switch,
        route_experts.T,
        out_gain,
        inner_gain,
        proj_step.T,
        conv_taps,
        earlier,
        step_bias,
        decay_rate,
        proj_x,
        proj_z,
        proj_b,
        proj_c,
        state,
        expert_gate,
        expert_up,
        expert_down,
        dense_gate,
        dense_up,
        dense_down,
    )
    return layer_out, new_state.reshape(scan_state.shape), new_conv.transpose(2, 0, 1, 3)


def on_device(
    resid,
    mix_gain,
    proj_x,
    proj_z,
    proj_b,
    proj_c,
    proj_step,
    step_bias,
    decay_rate,
    conv_taps,
    conv_state,
    scan_state,
    inner_gain,
    proj_out,
    post_gain,
    ffn_gain,
    group_router,
    expert_router,
    route_experts,
    expert_gate,
    expert_up,
    expert_down,
    dense_switch,
    dense_gate,
    dense_up,
    dense_down,
    out_gain,
):
    tp_index = lax.axis_index("tp")
    seqs = resid.shape[0]
    width = resid.shape[1]
    quarter = width // lax.axis_size("tp")
    heads_here = scan_state.shape[1]
    head_dim = scan_state.shape[2]
    state_dim = scan_state.shape[3]
    channels = conv_state.shape[3]
    repeat = heads_here // (channels // state_dim)
    whole_blocks = 2 * seqs * route_experts.shape[1] // expert_router.shape[1] >= seqs
    one_group = channels == state_dim == 128 and expert_router.shape[1] <= 64
    few = lax.axis_size("tp") == 4 and expert_gate.shape[0] == 1
    few = few and lax.axis_size("ep") % 2 == 0
    if whole_blocks and one_group and few:
        return fused_layer(
            resid,
            mix_gain,
            proj_x,
            proj_z,
            proj_b,
            proj_c,
            proj_step,
            step_bias,
            decay_rate,
            conv_taps,
            conv_state,
            scan_state,
            inner_gain,
            proj_out,
            post_gain,
            ffn_gain,
            group_router,
            expert_router,
            route_experts,
            expert_gate,
            expert_up,
            expert_down,
            dense_switch,
            dense_gate,
            dense_up,
            dense_down,
            out_gain,
        )
    normed = scaled_rows(resid, mix_gain).astype(jnp.bfloat16)
    fresh = jnp.stack(
        [
            jnp.dot(normed, proj_x, preferred_element_type=jnp.float32),
            jnp.dot(normed, proj_b, preferred_element_type=jnp.float32),
            jnp.dot(normed, proj_c, preferred_element_type=jnp.float32),
        ],
        axis=1,
    ).astype(jnp.bfloat16)
    gate_z = jnp.dot(normed, proj_z, preferred_element_type=jnp.float32)
    step_all = jnp.dot(normed, proj_step, preferred_element_type=jnp.float32)
    step_raw = lax.dynamic_slice_in_dim(step_all, tp_index * heads_here, heads_here, 1)
    history = jnp.concatenate([conv_state, fresh[:, :, None, :]], axis=2)
    activated = jax.nn.silu(
        jnp.sum(history.astype(jnp.float32) * conv_taps.astype(jnp.float32)[None], axis=2)
    )
    xs_heads = activated[:, 0].reshape(seqs, heads_here, head_dim)
    b_heads = jnp.repeat(activated[:, 1].reshape(seqs, -1, state_dim), repeat, axis=1)
    c_heads = jnp.repeat(activated[:, 2].reshape(seqs, -1, state_dim), repeat, axis=1)
    step = jax.nn.softplus(step_raw + step_bias)
    keep = jnp.exp(-decay_rate * step)
    driven = step[:, :, None] * xs_heads
    new_state = keep[:, :, None, None] * scan_state + driven[:, :, :, None] * b_heads[:, :, None, :]
    read = jnp.sum(new_state * c_heads[:, :, None, :], axis=3).reshape(seqs, channels)
    gated = (read * jax.nn.silu(gate_z) * inner_gain.astype(jnp.float32)).astype(jnp.bfloat16)
    new_conv = history[:, :, 1:, :]
    mixed = lax.psum(
        jnp.dot(gated, proj_out, preferred_element_type=jnp.float32).astype(jnp.bfloat16), "tp"
    ).astype(jnp.float32)
    stream = (resid.astype(jnp.float32) + scaled_rows(mixed, post_gain)).astype(jnp.bfloat16)
    feed = scaled_rows(stream, ffn_gain).astype(jnp.bfloat16)
    feed_quarter = lax.dynamic_slice_in_dim(feed, tp_index * quarter, quarter, 1)
    expert_count = expert_router.shape[1]
    group_size = expert_count // group_router.shape[1]
    pick_count = route_experts.shape[1]
    group_prob = softmax_plain(jnp.dot(feed, group_router, preferred_element_type=jnp.float32))
    expert_logits = jnp.dot(feed, expert_router, preferred_element_type=jnp.float32)
    matches = route_experts[:, :, None] == jnp.arange(expert_count, dtype=jnp.int32)[None, None, :]
    pick_logits = jnp.sum(jnp.where(matches, expert_logits[:, None, :], 0.0), axis=2)
    chosen_group = route_experts[:, 0] // group_size
    group_ids = jnp.arange(group_router.shape[1], dtype=jnp.int32)
    group_weight = jnp.sum(
        jnp.where(chosen_group[:, None] == group_ids[None, :], group_prob, 0.0), axis=1
    )
    pick_weight = softmax_plain(pick_logits) * group_weight[:, None]
    capacity = 2 * seqs * pick_count // expert_count
    flat_picks = route_experts.reshape(-1)
    one_hot = (flat_picks[:, None] == jnp.arange(expert_count, dtype=jnp.int32)[None, :]).astype(
        jnp.int32
    )
    slot = jnp.sum((jnp.cumsum(one_hot, axis=0) - one_hot) * one_hot, axis=1)
    target = flat_picks * capacity + slot
    repeated = jnp.repeat(feed, pick_count, axis=0)
    outgoing = jnp.zeros((expert_count * capacity, width), jnp.bfloat16).at[target].set(repeated)
    outgoing = outgoing.reshape(expert_count, capacity, width)
    arrived = lax.all_to_all(outgoing, "ep", split_axis=0, concat_axis=0, tiled=True)
    sources = arrived.shape[0]
    items = arrived.shape[1]
    rows = arrived.reshape(sources * items, width)
    gate_value = jnp.dot(rows, expert_gate[0], preferred_element_type=jnp.float32)
    up_value = jnp.dot(rows, expert_up[0], preferred_element_type=jnp.float32)
    hidden = (jax.nn.silu(gate_value) * up_value).astype(jnp.bfloat16)
    result = jnp.dot(hidden, expert_down[0], preferred_element_type=jnp.float32).reshape(
        sources, items, width
    )
    summed = lax.psum_scatter(result.astype(jnp.bfloat16), "tp", scatter_dimension=2, tiled=True)
    returned = lax.all_to_all(summed, "ep", split_axis=0, concat_axis=0, tiled=True)
    fetched = returned.reshape(expert_count * capacity, quarter)[target].reshape(
        seqs, pick_count, quarter
    )
    routed = jnp.sum(fetched.astype(jnp.float32) * pick_weight[:, :, None], axis=1)
    gate_piece = jnp.einsum(
        "sd,cd->sc",
        feed_quarter,
        lax.all_gather(dense_gate, "ep", axis=0, tiled=True),
        preferred_element_type=jnp.float32,
    )
    up_piece = jnp.einsum(
        "sd,cd->sc",
        feed_quarter,
        lax.all_gather(dense_up, "ep", axis=0, tiled=True),
        preferred_element_type=jnp.float32,
    )
    gate_sum = gate_piece
    up_sum = up_piece
    gate_sum, up_sum = (
        lax.psum(gate_sum.astype(jnp.bfloat16), "tp").astype(jnp.float32),
        lax.psum(up_sum.astype(jnp.bfloat16), "tp").astype(jnp.float32),
    )
    dense_hidden = (jax.nn.silu(gate_sum) * up_sum).astype(jnp.bfloat16)
    dense_out = jnp.dot(
        dense_hidden,
        lax.all_gather(dense_down, "ep", axis=0, tiled=True),
        preferred_element_type=jnp.float32,
    )
    switch = jax.nn.sigmoid(jnp.dot(feed, dense_switch, preferred_element_type=jnp.float32))
    combined = routed + switch[:, None] * dense_out
    total_square = lax.psum(jnp.sum(combined * combined, axis=1), "tp")
    scale = lax.rsqrt(total_square / width + norm_eps)
    stream_part = lax.dynamic_slice_in_dim(stream, tp_index * quarter, quarter, 1).astype(
        jnp.float32
    )
    layer_out = (stream_part + combined * scale[:, None] * out_gain.astype(jnp.float32)).astype(
        jnp.bfloat16
    )
    return (layer_out, new_state, new_conv)


def solution(mesh):
    placed = (
        P("ep", None),
        P(),
        P(None, "tp"),
        P(None, "tp"),
        P(None, "tp"),
        P(None, "tp"),
        P(),
        P("tp"),
        P("tp"),
        P(None, None, "tp"),
        P("ep", None, None, "tp"),
        P("ep", "tp", None, None),
        P("tp"),
        P("tp", None),
        P(),
        P(),
        P(),
        P(),
        P("ep", None),
        P("ep", None, "tp"),
        P("ep", None, "tp"),
        P("ep", "tp", None),
        P(),
        P("ep", "tp"),
        P("ep", "tp"),
        P("ep", "tp"),
        P("tp"),
    )
    return jax.shard_map(
        on_device,
        mesh=mesh,
        in_specs=placed,
        out_specs=(P("ep", "tp"), P("ep", "tp", None, None), P("ep", None, None, "tp")),
        check_vma=False,
    )
```

```python
import functools

import jax
import jax.numpy as jnp
from jax import lax
from jax.experimental import pallas as pl
from jax.experimental.pallas import tpu as pltpu
from jax.sharding import PartitionSpec as P

norm_eps = 1e-06


def scaled_rows(values, gain):
    values = values.astype(jnp.float32)
    mean_square = jnp.mean(values * values, axis=-1, keepdims=True)
    return values * lax.rsqrt(mean_square + norm_eps) * gain.astype(jnp.float32)


def softmax_plain(logits):
    weights = jnp.exp(logits)
    return weights / jnp.sum(weights, axis=-1, keepdims=True)


def fused_kernel(
    ep,
    group_size,
    group_count,
    expert_count,
    proj_out_ref,
    resid_ref,
    mix_ref,
    post_ref,
    ffn_ref,
    expert_router_ref,
    group_router_ref,
    switch_ref,
    route_ref,
    out_gain_ref,
    inner_ref,
    proj_step_ref,
    taps_ref,
    conv_ref,
    bias_ref,
    decay_ref,
    proj_x_hbm,
    proj_z_hbm,
    proj_b_hbm,
    proj_c_hbm,
    state_hbm,
    gate_hbm,
    up_hbm,
    down_hbm,
    dense_gate_hbm,
    dense_up_hbm,
    dense_down_hbm,
    out_ref,
    new_state_ref,
    new_conv_ref,
    proj_w,
    state_buf,
    router_buf,
    gate_w,
    up_w,
    down_w,
    dgate,
    dup,
    ddown,
    stream_buf,
    mix_own,
    mix_peer,
    half_own,
    half_far,
    rows_buf,
    aux_buf,
    part_buf,
    part_peer,
    send_x,
    recv_x,
    send_ep,
    recv_ep,
    square_own,
    square_peer,
    local_sem,
    dense_send,
    dense_recv,
    mix_send,
    mix_recv,
    rows_send,
    rows_recv,
    aux_send,
    aux_recv,
    part_send,
    part_recv,
    x_send,
    x_recv,
    ep_send,
    ep_recv,
    square_send,
    square_recv,
    entered,
    z_send,
    z_aux_send,
):
    f32, bf16 = jnp.float32, jnp.bfloat16
    me = lax.axis_index("ep")
    tp = lax.axis_index("tp")
    far = tp // 2
    core = tp % 2
    beside = far * 2 + (1 - core)
    across = (1 - far) * 2 + core
    diagonal = (1 - far) * 2 + (1 - core)
    near = (beside, across, diagonal)
    seqs, width = resid_ref.shape
    quarter = width // 4
    share = dgate.shape[1]

    def remote(src, dst, send, recv, ep_to, tp_to):
        return pltpu.make_async_remote_copy(
            src_ref=src,
            dst_ref=dst,
            send_sem=send,
            recv_sem=recv,
            device_id=(ep_to, tp_to),
            device_id_type=pl.DeviceIdType.MESH,
        )

    def ep_at(step):
        return lax.rem(me + step + ep, ep)

    local = []

    def load(src, dst):
        copy = pltpu.make_async_copy(src, dst, local_sem.at[len(local)])
        copy.start()
        local.append(copy)

    for k, src in enumerate((proj_x_hbm, proj_b_hbm, proj_c_hbm, proj_z_hbm)):
        load(src, proj_w.at[k])
    load(state_hbm, state_buf)
    load(gate_hbm.at[0], gate_w)
    load(up_hbm.at[0], up_w)
    for q in range(4):
        load(down_hbm.at[0, :, pl.ds(q * quarter, quarter)], down_w.at[q])
    dense_pairs = ((dense_gate_hbm, dgate), (dense_up_hbm, dup), (dense_down_hbm, ddown))
    for src, dst in dense_pairs:
        load(src.at[pl.ds(tp * share, share), :], dst.at[tp])

    barrier = pltpu.get_barrier_semaphore()
    for step in range(1, ep):

        @pl.when(me + step < ep)
        def _():
            pl.semaphore_signal(
                barrier, inc=1, device_id=(ep_at(step), tp), device_id_type=pl.DeviceIdType.MESH
            )

    for peer in near:
        pl.semaphore_signal(
            barrier, inc=1, device_id=(me, peer), device_id_type=pl.DeviceIdType.MESH
        )

    def row(ref):
        return ref[...].astype(f32).reshape(1, ref.shape[0])

    resid_f = resid_ref[...].astype(f32)
    resid_scale = lax.rsqrt(jnp.mean(resid_f * resid_f, axis=1, keepdims=True) + norm_eps)
    normed = (resid_f * resid_scale * row(mix_ref)).astype(bf16)
    group_base = -(-expert_count // 8) * 8
    switch_lane = group_base + -(-group_count // 8) * 8
    router_buf[...] = jnp.zeros_like(router_buf)
    router_buf[0:expert_count, :] = expert_router_ref[...].astype(f32)
    router_buf[group_base : group_base + group_count, :] = group_router_ref[...].astype(f32)
    router_buf[switch_lane : switch_lane + 1, :] = row(switch_ref)
    nt = (((1,), (1,)), ((), ()))
    step_all = lax.dot_general(normed, proj_step_ref[...], nt, preferred_element_type=f32)
    pl.semaphore_wait(barrier, me + 3)
    for step in range(1, ep):

        @pl.when(me >= step)
        def _():
            pl.semaphore_signal(
                entered, inc=1, device_id=(me - step, tp), device_id_type=pl.DeviceIdType.MESH
            )


    sends = []
    dense_copies = []

    def send_dense(t):
        src, dst = dense_pairs[t]
        for k, peer in enumerate(near):
            copy = remote(
                src.at[pl.ds(peer * share, share), :],
                dst.at[tp],
                dense_send.at[3 * t + k],
                dense_recv.at[3 * t + k],
                me,
                peer,
            )
            copy.start()
            dense_copies.append(copy)

    send_dense(0)
    send_dense(1)

    channels = conv_ref.shape[3]
    heads = bias_ref.shape[0]
    head_dim = channels // heads
    taps = taps_ref[...].astype(f32)
    old = conv_ref.shape[1]
    active = []
    for k in range(3):
        local[k].wait()
        fresh = jnp.dot(normed, proj_w[k], preferred_element_type=f32).astype(bf16)
        summed = conv_ref[k, 0].astype(f32) * taps[k, 0:1]
        for tap in range(1, old):
            earlier = conv_ref[k, tap]
            new_conv_ref[k, tap - 1] = earlier
            summed = summed + earlier.astype(f32) * taps[k, tap : tap + 1]
        new_conv_ref[k, old - 1] = fresh
        summed = summed + fresh.astype(f32) * taps[k, old : old + 1]
        active.append(summed * jax.nn.sigmoid(summed))
    inputs, vec_in, vec_read = active
    local[3].wait()
    gate_z = jnp.dot(normed, proj_w[3], preferred_element_type=f32)
    step_lane = lax.broadcasted_iota(jnp.int32, step_all.shape, 1)
    lane_in = lax.broadcasted_iota(jnp.int32, (seqs, channels), 1)
    keep = jnp.zeros((seqs, channels), f32)
    stepped = jnp.zeros((seqs, channels), f32)
    for h in range(heads):
        raw = jnp.sum(
            jnp.where(step_lane == tp * heads + h, step_all, 0.0), axis=1, keepdims=True
        )
        raw = raw + bias_ref[h]
        step = jnp.maximum(raw, 0.0) + jnp.log1p(jnp.exp(-jnp.abs(raw)))
        mine = (lane_in >= h * head_dim) & (lane_in < (h + 1) * head_dim)
        keep = jnp.where(mine, jnp.exp(-decay_ref[h] * step), keep)
        stepped = jnp.where(mine, step, stepped)
    columns = jnp.concatenate(
        [keep, stepped * inputs, jnp.zeros((channels - 2 * seqs, channels), f32)], axis=0
    ).T
    local[4].wait()
    read_lane = lax.broadcasted_iota(jnp.int32, (channels, channels), 1)
    read = jnp.zeros((channels, channels), f32)
    for t in range(seqs):
        fresh_state = (
            columns[:, t : t + 1] * state_buf[t]
            + columns[:, seqs + t : seqs + t + 1] * vec_in[t : t + 1]
        )
        new_state_ref[t] = fresh_state
        value = jnp.sum(fresh_state * vec_read[t : t + 1], axis=1, keepdims=True)
        read = jnp.where(read_lane == t, value, read)
    read = read.T[0:seqs]
    gated = (read * (gate_z * jax.nn.sigmoid(gate_z)) * row(inner_ref)).astype(bf16)
    mix_own[...] = jnp.dot(gated, proj_out_ref[...], preferred_element_type=f32).astype(bf16)

    first = remote(mix_own, mix_peer, mix_send.at[0], mix_recv.at[0], me, beside)
    first.start()
    sends.append(first)
    first.wait_recv()
    half = width // 2
    chip_sum = (mix_own[...].astype(f32) + mix_peer[...].astype(f32)).astype(bf16)
    half_own[0] = chip_sum[:, :half]
    half_own[1] = chip_sum[:, half:]
    over_x = remote(
        half_own.at[core], half_far.at[core], mix_send.at[1], mix_recv.at[1], me, across
    )
    over_x.start()
    send_dense(2)
    sends += dense_copies

    over_x.wait_recv()
    to_core = remote(
        half_far.at[core], half_far.at[core], mix_send.at[2], mix_recv.at[2], me, beside
    )
    to_core.start()
    sends += [over_x, to_core]
    to_core.wait_recv()

    far_sum = jnp.concatenate([half_far[0], half_far[1]], axis=1)
    mixed = chip_sum.astype(f32) + far_sum.astype(f32)
    mixed_scale = lax.rsqrt(jnp.mean(mixed * mixed, axis=1, keepdims=True) + norm_eps)
    stream = (
        resid_f + mixed * mixed_scale * row(post_ref)
    ).astype(bf16)
    stream_f = stream.astype(f32)
    feed_scale = lax.rsqrt(jnp.mean(stream_f * stream_f, axis=1, keepdims=True) + norm_eps)
    feed_f = stream_f * feed_scale * row(ffn_ref)
    feed = feed_f.astype(bf16)
    my_z, my_y = me // 2, me % 2
    nz = ep // 2
    here = my_y * nz + my_z

    def feed_of(q):
        value = feed_f[:, :quarter]
        for other in range(1, 4):
            piece = feed_f[:, other * quarter : (other + 1) * quarter]
            value = jnp.where(q == other, piece, value)
        return value.astype(bf16)

    quarters = (tp, beside, across, diagonal)
    for k, q in enumerate(quarters):
        rows_buf[k, here] = feed_of(q)
    for q in range(4):
        stream_buf[q] = stream[:, q * quarter : (q + 1) * quarter]

    @pl.when(me + 1 < ep)
    def _():
        pl.semaphore_wait(entered, ep - 1 - me)

    def other(j):
        return j + (j - my_z + nz) // nz

    others = [other(j) for j in range(nz - 1)]
    upper = my_z // (nz // 2)
    far_first = [other(upper * j + (1 - upper) * (nz - 2 - j)) for j in range(nz - 1)]

    def rows_copy(k, at, send, ep_to, tp_to, k_to):
        return remote(
            rows_buf.at[k, at],
            rows_buf.at[k_to, at],
            rows_send.at[send, at],
            rows_recv.at[k_to, at],
            ep_to,
            tp_to,
        )

    def aux_copy(at, send, ep_to):
        return remote(
            aux_buf.at[at], aux_buf.at[at], aux_send.at[send, at], aux_recv.at[at], ep_to, tp
        )

    def z_rows(z):
        return remote(
            rows_buf.at[0, here],
            rows_buf.at[0, here],
            z_send.at[z],
            rows_recv.at[0, here],
            z * 2 + my_y,
            tp,
        )

    def z_aux(z):
        return remote(
            aux_buf.at[here], aux_buf.at[here], z_aux_send.at[z], aux_recv.at[here],
            z * 2 + my_y, tp,
        )

    def started(copy):
        copy.start()
        sends.append(copy)

    for z in far_first:
        started(z_rows(z))
    over_y = my_z * 2 + 1 - my_y
    started(rows_copy(0, here, 0, over_y, tp, 0))
    started(rows_copy(2, here, 1, over_y, tp, 2))

    logits = lax.dot_general(
        feed, router_buf[...].astype(bf16), nt, preferred_element_type=f32
    )
    lane = lax.broadcasted_iota(jnp.int32, logits.shape, 1)
    same = lax.broadcasted_iota(jnp.int32, (seqs, seqs), 0) == lax.broadcasted_iota(
        jnp.int32, (seqs, seqs), 1
    )
    route = lax.dot_general(
        jnp.where(same, 1.0, 0.0).astype(bf16),
        route_ref[...].astype(f32).astype(bf16),
        nt,
        preferred_element_type=f32,
    ).astype(jnp.int32)
    picked = lane == route[:, 0:1]
    for k in range(1, route.shape[1]):
        picked = picked | (lane == route[:, k : k + 1])
    weights = jnp.exp(logits)
    pick = jnp.where(picked, weights, 0.0)
    group_lane = (lane - group_base) * group_size
    in_groups = (lane >= group_base) & (lane < group_base + group_count)
    group = jnp.where(in_groups, weights, 0.0)
    lead = route[:, 0:1]
    chosen = in_groups & (lead >= group_lane) & (lead < group_lane + group_size)
    group_weight = jnp.sum(jnp.where(chosen, weights, 0.0), axis=1, keepdims=True) / jnp.sum(
        group, axis=1, keepdims=True
    )
    pick = pick / jnp.sum(pick, axis=1, keepdims=True) * group_weight
    aux_buf[here] = jnp.where(lane == switch_lane, jax.nn.sigmoid(logits), pick).astype(bf16)
    for z in far_first:
        started(z_aux(z))
    started(aux_copy(here, 0, over_y))

    total = nz * seqs
    sides = (my_y, 1 - my_y)

    def at_of(side, z):
        return sides[side] * nz + z

    def arrived(k, at):
        rows_copy(k, at, 0, me, beside, k).wait_recv()

    there = at_of(1, my_z)
    for z in others:
        at = at_of(0, z)
        arrived(0, at)
        started(rows_copy(0, at, 0, over_y, tp, 0))
        started(rows_copy(0, at, 1, me, across, 2))
        started(rows_copy(0, at, 2, me, beside, 1))
    arrived(0, there)
    started(rows_copy(0, there, 2, me, beside, 1))
    arrived(2, there)
    started(rows_copy(2, there, 3, me, beside, 3))
    for z in others:
        at = at_of(0, z)
        aux_copy(at, 0, me).wait_recv()
        started(aux_copy(at, 0, over_y))
    for z in others:
        at = at_of(1, z)
        arrived(0, at)
        started(rows_copy(0, at, 1, me, across, 2))
        started(rows_copy(0, at, 2, me, beside, 1))
    for z in others:
        at = at_of(0, z)
        arrived(2, at)
        started(rows_copy(2, at, 3, me, beside, 3))

    def gather_end(side):
        for z in range(nz) if side else others:
            at = at_of(side, z)
            if side:
                aux_copy(at, 0, me).wait_recv()
            arrived(1, at)
            arrived(3, at)

    def add(total_sum, value):
        return value if total_sum is None else total_sum + value

    def part_copy(k, side):
        block = pl.ds(sides[side] * nz, nz)
        return remote(
            part_buf.at[(diagonal, beside)[k], block],
            part_peer.at[k, block],
            part_send.at[k, side],
            part_recv.at[k, side],
            me,
            beside,
        )

    def feed_forward(side):
        block = pl.ds(sides[side] * nz, nz)
        gate = up = dense_g = dense_u = None
        for k, q in enumerate(quarters):
            rows = rows_buf[k, block].reshape(total, quarter)
            span = pl.ds(pl.multiple_of(q * quarter, quarter), quarter)
            gate = add(gate, jnp.dot(rows, gate_w[span, :], preferred_element_type=f32))
            up = add(up, jnp.dot(rows, up_w[span, :], preferred_element_type=f32))
            dense_g = add(
                dense_g, lax.dot_general(rows, dgate[q], nt, preferred_element_type=f32)
            )
            dense_u = add(dense_u, lax.dot_general(rows, dup[q], nt, preferred_element_type=f32))
        aux = aux_buf[block].reshape(total, aux_buf.shape[2]).astype(f32)
        aux_lane = lax.broadcasted_iota(jnp.int32, aux.shape, 1)
        weight = jnp.sum(jnp.where(aux_lane == me, aux, 0.0), axis=1, keepdims=True)
        switch = jnp.sum(jnp.where(aux_lane == switch_lane, aux, 0.0), axis=1, keepdims=True)
        hidden = (gate * jax.nn.sigmoid(gate) * up * weight).astype(bf16)
        dense_hidden = (dense_g * jax.nn.sigmoid(dense_g) * dense_u * switch).astype(bf16)
        for k, q in enumerate((diagonal, beside, across, tp)):
            value = jnp.dot(hidden, down_w[q], preferred_element_type=f32) + jnp.dot(
                dense_hidden, ddown[q], preferred_element_type=f32
            )
            part_buf[q, block] = value.astype(bf16).reshape(nz, seqs, quarter)
            if k < 2:
                started(part_copy(k, side))

    far_then_own = far_first + [my_z]

    def x_copy(at):
        return remote(send_x.at[at], recv_x.at[at], x_send.at[at], x_recv.at[at], me, across)

    def sums_over_x(side):
        part_copy(0, side).wait_recv()
        for z in far_then_own:
            at = at_of(side, z)
            send_x[at] = (
                part_buf[across, at].astype(f32) + part_peer[0, at].astype(f32)
            ).astype(bf16)
            started(x_copy(at))

    def ep_copy(at, slot, ep_to):
        return remote(
            send_ep.at[at], recv_ep.at[slot], ep_send.at[at], ep_recv.at[slot], ep_to, tp
        )

    def summed(at):
        x_copy(at).wait_recv()
        return (
            part_buf[tp, at].astype(f32)
            + part_peer[1, at].astype(f32)
            + recv_x[at].astype(f32)
        )

    def sums_over_ep(side):
        part_copy(1, side).wait_recv()
        for z in far_then_own if side else far_first:
            at = at_of(side, z)
            send_ep[at] = summed(at).astype(bf16)
            started(ep_copy(at, here, z * 2 + sides[side]))

    for copy in local[5:]:
        copy.wait()
    for copy in dense_copies:
        copy.wait_recv()
    gather_end(0)
    feed_forward(0)
    for z in others:
        at = at_of(1, z)
        arrived(2, at)
        started(rows_copy(2, at, 3, me, beside, 3))
    sums_over_x(0)
    gather_end(1)
    feed_forward(1)
    sums_over_ep(0)
    sums_over_x(1)
    combined = summed(here)
    sums_over_ep(1)

    for side in range(2):
        for z in range(nz) if side else others:
            at = at_of(side, z)
            ep_copy(at, at, me).wait_recv()
            combined = combined + recv_ep[at].astype(f32)

    square = jnp.sum(combined * combined, axis=1, keepdims=True)
    lanes = square_own.shape[1]
    row_id = lax.broadcasted_iota(jnp.int32, (seqs, lanes), 0)
    diagonal_lane = row_id == lax.broadcasted_iota(jnp.int32, (seqs, lanes), 1)
    square_row = jnp.sum(jnp.where(diagonal_lane, square, 0.0), axis=0, keepdims=True)
    square_own[...] = jnp.broadcast_to(square_row, square_own.shape)
    square_copies = []
    for k, peer in enumerate(near):
        copy = remote(
            square_own, square_peer.at[k], square_send.at[k], square_recv.at[k], me, peer
        )
        copy.start()
        square_copies.append(copy)
    sends += square_copies
    for copy in square_copies:
        copy.wait_recv()
    everything = (square_own[...] + square_peer[0]) + (square_peer[1] + square_peer[2])
    spread = jnp.where(diagonal_lane, everything[0:1], 0.0)
    scale = lax.rsqrt(jnp.sum(spread, axis=1, keepdims=True) / width + norm_eps)
    own_stream = stream_buf[tp].astype(f32)
    out_ref[...] = (own_stream + combined * scale * row(out_gain_ref)).astype(bf16)
    for copy in sends:
        copy.wait_send()


def write_kernel(out_ref, state_ref, conv_ref, out_hbm, state_hbm, conv_hbm, sems):
    pairs = ((state_ref, state_hbm), (conv_ref, conv_hbm), (out_ref, out_hbm))
    copies = [pltpu.make_async_copy(src, dst, sems.at[k]) for k, (src, dst) in enumerate(pairs)]
    for copy in copies:
        copy.start()
    for copy in copies:
        copy.wait()


def fused_layer(
    resid,
    mix_gain,
    proj_x,
    proj_z,
    proj_b,
    proj_c,
    proj_step,
    step_bias,
    decay_rate,
    conv_taps,
    conv_state,
    scan_state,
    inner_gain,
    proj_out,
    post_gain,
    ffn_gain,
    group_router,
    expert_router,
    route_experts,
    expert_gate,
    expert_up,
    expert_down,
    dense_switch,
    dense_gate,
    dense_up,
    dense_down,
    out_gain,
):
    ep = lax.axis_size("ep")
    seqs, width = resid.shape
    quarter = width // 4
    channels = conv_state.shape[3]
    expert_count = expert_router.shape[1]
    group_count = group_router.shape[1]
    lanes = 128
    hidden_here = expert_gate.shape[2]
    share = dense_gate.shape[0] // 4
    bf16 = jnp.bfloat16
    vmem = pl.BlockSpec(memory_space=pltpu.VMEM)
    hbm = pl.BlockSpec(memory_space=pl.ANY)
    dma = pltpu.SemaphoreType.DMA
    kernel = functools.partial(
        fused_kernel, ep, expert_count // group_count, group_count, expert_count
    )
    smem = pl.BlockSpec(memory_space=pltpu.SMEM)
    earlier = conv_state.transpose(1, 2, 0, 3)
    state = scan_state.reshape(seqs, channels, scan_state.shape[3])
    results = pl.pallas_call(
        kernel,
        out_shape=(
            pltpu.VMEM((seqs, quarter), bf16),
            pltpu.VMEM(state.shape, state.dtype),
            pltpu.VMEM(earlier.shape, earlier.dtype),
        ),
        in_specs=[vmem] * 14 + [smem] * 2 + [hbm] * 11,
        out_specs=(vmem, vmem, vmem),
        scratch_shapes=[
            pltpu.VMEM((4,) + proj_x.shape, bf16),
            pltpu.VMEM(state.shape, state.dtype),
            pltpu.VMEM((lanes, width), jnp.float32),
            pltpu.VMEM((width, hidden_here), bf16),
            pltpu.VMEM((width, hidden_here), bf16),
            pltpu.VMEM((4, hidden_here, quarter), bf16),
            pltpu.VMEM((4, share, quarter), bf16),
            pltpu.VMEM((4, share, quarter), bf16),
            pltpu.VMEM((4, share, quarter), bf16),
            pltpu.VMEM((4, seqs, quarter), bf16),
            pltpu.VMEM((seqs, width), bf16),
            pltpu.VMEM((seqs, width), bf16),
            pltpu.VMEM((2, seqs, width // 2), bf16),
            pltpu.VMEM((2, seqs, width // 2), bf16),
            pltpu.VMEM((4, ep, seqs, quarter), bf16),
            pltpu.VMEM((ep, seqs, lanes), bf16),
            pltpu.VMEM((4, ep, seqs, quarter), bf16),
            pltpu.VMEM((2, ep, seqs, quarter), bf16),
            pltpu.VMEM((ep, seqs, quarter), bf16),
            pltpu.VMEM((ep, seqs, quarter), bf16),
            pltpu.VMEM((ep, seqs, quarter), bf16),
            pltpu.VMEM((ep, seqs, quarter), bf16),
            pltpu.VMEM((8, lanes), jnp.float32),
            pltpu.VMEM((3, 8, lanes), jnp.float32),
            dma((14,)),
            dma((9,)),
            dma((9,)),
            dma((3,)),
            dma((3,)),
            dma((4, ep)),
            dma((4, ep)),
            dma((1, ep)),
            dma((ep,)),
            dma((2, 2)),
            dma((2, 2)),
            dma((ep,)),
            dma((ep,)),
            dma((ep,)),
            dma((ep,)),
            dma((3,)),
            dma((3,)),
            pltpu.SemaphoreType.REGULAR,
            dma((ep,)),
            dma((ep,)),
        ],
        compiler_params=pltpu.CompilerParams(collective_id=0, has_side_effects=True),
        name="fused_layer",
    )(
        proj_out,
        resid,
        mix_gain,
        post_gain,
        ffn_gain,
        expert_router.T,
        group_router.T,
        dense_switch,
        route_experts.T,
        out_gain,
        inner_gain,
        proj_step.T,
        conv_taps,
        earlier,
        step_bias,
        decay_rate,
        proj_x,
        proj_z,
        proj_b,
        proj_c,
        state,
        expert_gate,
        expert_up,
        expert_down,
        dense_gate,
        dense_up,
        dense_down,
    )
    layer_out, new_state, new_conv = pl.pallas_call(
        write_kernel,
        out_shape=tuple(jax.ShapeDtypeStruct(one.shape, one.dtype) for one in results),
        in_specs=[vmem] * 3,
        out_specs=(hbm, hbm, hbm),
        scratch_shapes=[dma((3,))],
        compiler_params=pltpu.CompilerParams(vmem_limit_bytes=4 << 20),
        name="write_results",
    )(*results)
    return layer_out, new_state.reshape(scan_state.shape), new_conv.transpose(2, 0, 1, 3)


def on_device(
    resid,
    mix_gain,
    proj_x,
    proj_z,
    proj_b,
    proj_c,
    proj_step,
    step_bias,
    decay_rate,
    conv_taps,
    conv_state,
    scan_state,
    inner_gain,
    proj_out,
    post_gain,
    ffn_gain,
    group_router,
    expert_router,
    route_experts,
    expert_gate,
    expert_up,
    expert_down,
    dense_switch,
    dense_gate,
    dense_up,
    dense_down,
    out_gain,
):
    tp_index = lax.axis_index("tp")
    seqs = resid.shape[0]
    width = resid.shape[1]
    quarter = width // lax.axis_size("tp")
    heads_here = scan_state.shape[1]
    head_dim = scan_state.shape[2]
    state_dim = scan_state.shape[3]
    channels = conv_state.shape[3]
    repeat = heads_here // (channels // state_dim)
    whole_blocks = 2 * seqs * route_experts.shape[1] // expert_router.shape[1] >= seqs
    one_group = channels == state_dim == 128 and expert_router.shape[1] <= 64
    few = lax.axis_size("tp") == 4 and expert_gate.shape[0] == 1
    few = few and lax.axis_size("ep") % 2 == 0
    if whole_blocks and one_group and few:
        return fused_layer(
            resid,
            mix_gain,
            proj_x,
            proj_z,
            proj_b,
            proj_c,
            proj_step,
            step_bias,
            decay_rate,
            conv_taps,
            conv_state,
            scan_state,
            inner_gain,
            proj_out,
            post_gain,
            ffn_gain,
            group_router,
            expert_router,
            route_experts,
            expert_gate,
            expert_up,
            expert_down,
            dense_switch,
            dense_gate,
            dense_up,
            dense_down,
            out_gain,
        )
    normed = scaled_rows(resid, mix_gain).astype(jnp.bfloat16)
    fresh = jnp.stack(
        [
            jnp.dot(normed, proj_x, preferred_element_type=jnp.float32),
            jnp.dot(normed, proj_b, preferred_element_type=jnp.float32),
            jnp.dot(normed, proj_c, preferred_element_type=jnp.float32),
        ],
        axis=1,
    ).astype(jnp.bfloat16)
    gate_z = jnp.dot(normed, proj_z, preferred_element_type=jnp.float32)
    step_all = jnp.dot(normed, proj_step, preferred_element_type=jnp.float32)
    step_raw = lax.dynamic_slice_in_dim(step_all, tp_index * heads_here, heads_here, 1)
    history = jnp.concatenate([conv_state, fresh[:, :, None, :]], axis=2)
    activated = jax.nn.silu(
        jnp.sum(history.astype(jnp.float32) * conv_taps.astype(jnp.float32)[None], axis=2)
    )
    xs_heads = activated[:, 0].reshape(seqs, heads_here, head_dim)
    b_heads = jnp.repeat(activated[:, 1].reshape(seqs, -1, state_dim), repeat, axis=1)
    c_heads = jnp.repeat(activated[:, 2].reshape(seqs, -1, state_dim), repeat, axis=1)
    step = jax.nn.softplus(step_raw + step_bias)
    keep = jnp.exp(-decay_rate * step)
    driven = step[:, :, None] * xs_heads
    new_state = keep[:, :, None, None] * scan_state + driven[:, :, :, None] * b_heads[:, :, None, :]
    read = jnp.sum(new_state * c_heads[:, :, None, :], axis=3).reshape(seqs, channels)
    gated = (read * jax.nn.silu(gate_z) * inner_gain.astype(jnp.float32)).astype(jnp.bfloat16)
    new_conv = history[:, :, 1:, :]
    mixed = lax.psum(
        jnp.dot(gated, proj_out, preferred_element_type=jnp.float32).astype(jnp.bfloat16), "tp"
    ).astype(jnp.float32)
    stream = (resid.astype(jnp.float32) + scaled_rows(mixed, post_gain)).astype(jnp.bfloat16)
    feed = scaled_rows(stream, ffn_gain).astype(jnp.bfloat16)
    feed_quarter = lax.dynamic_slice_in_dim(feed, tp_index * quarter, quarter, 1)
    expert_count = expert_router.shape[1]
    group_size = expert_count // group_router.shape[1]
    pick_count = route_experts.shape[1]
    group_prob = softmax_plain(jnp.dot(feed, group_router, preferred_element_type=jnp.float32))
    expert_logits = jnp.dot(feed, expert_router, preferred_element_type=jnp.float32)
    matches = route_experts[:, :, None] == jnp.arange(expert_count, dtype=jnp.int32)[None, None, :]
    pick_logits = jnp.sum(jnp.where(matches, expert_logits[:, None, :], 0.0), axis=2)
    chosen_group = route_experts[:, 0] // group_size
    group_ids = jnp.arange(group_router.shape[1], dtype=jnp.int32)
    group_weight = jnp.sum(
        jnp.where(chosen_group[:, None] == group_ids[None, :], group_prob, 0.0), axis=1
    )
    pick_weight = softmax_plain(pick_logits) * group_weight[:, None]
    capacity = 2 * seqs * pick_count // expert_count
    flat_picks = route_experts.reshape(-1)
    one_hot = (flat_picks[:, None] == jnp.arange(expert_count, dtype=jnp.int32)[None, :]).astype(
        jnp.int32
    )
    slot = jnp.sum((jnp.cumsum(one_hot, axis=0) - one_hot) * one_hot, axis=1)
    target = flat_picks * capacity + slot
    repeated = jnp.repeat(feed, pick_count, axis=0)
    outgoing = jnp.zeros((expert_count * capacity, width), jnp.bfloat16).at[target].set(repeated)
    outgoing = outgoing.reshape(expert_count, capacity, width)
    arrived = lax.all_to_all(outgoing, "ep", split_axis=0, concat_axis=0, tiled=True)
    sources = arrived.shape[0]
    items = arrived.shape[1]
    rows = arrived.reshape(sources * items, width)
    gate_value = jnp.dot(rows, expert_gate[0], preferred_element_type=jnp.float32)
    up_value = jnp.dot(rows, expert_up[0], preferred_element_type=jnp.float32)
    hidden = (jax.nn.silu(gate_value) * up_value).astype(jnp.bfloat16)
    result = jnp.dot(hidden, expert_down[0], preferred_element_type=jnp.float32).reshape(
        sources, items, width
    )
    summed = lax.psum_scatter(result.astype(jnp.bfloat16), "tp", scatter_dimension=2, tiled=True)
    returned = lax.all_to_all(summed, "ep", split_axis=0, concat_axis=0, tiled=True)
    fetched = returned.reshape(expert_count * capacity, quarter)[target].reshape(
        seqs, pick_count, quarter
    )
    routed = jnp.sum(fetched.astype(jnp.float32) * pick_weight[:, :, None], axis=1)
    gate_piece = jnp.einsum(
        "sd,cd->sc",
        feed_quarter,
        lax.all_gather(dense_gate, "ep", axis=0, tiled=True),
        preferred_element_type=jnp.float32,
    )
    up_piece = jnp.einsum(
        "sd,cd->sc",
        feed_quarter,
        lax.all_gather(dense_up, "ep", axis=0, tiled=True),
        preferred_element_type=jnp.float32,
    )
    gate_sum = gate_piece
    up_sum = up_piece
    gate_sum, up_sum = (
        lax.psum(gate_sum.astype(jnp.bfloat16), "tp").astype(jnp.float32),
        lax.psum(up_sum.astype(jnp.bfloat16), "tp").astype(jnp.float32),
    )
    dense_hidden = (jax.nn.silu(gate_sum) * up_sum).astype(jnp.bfloat16)
    dense_out = jnp.dot(
        dense_hidden,
        lax.all_gather(dense_down, "ep", axis=0, tiled=True),
        preferred_element_type=jnp.float32,
    )
    switch = jax.nn.sigmoid(jnp.dot(feed, dense_switch, preferred_element_type=jnp.float32))
    combined = routed + switch[:, None] * dense_out
    total_square = lax.psum(jnp.sum(combined * combined, axis=1), "tp")
    scale = lax.rsqrt(total_square / width + norm_eps)
    stream_part = lax.dynamic_slice_in_dim(stream, tp_index * quarter, quarter, 1).astype(
        jnp.float32
    )
    layer_out = (stream_part + combined * scale[:, None] * out_gain.astype(jnp.float32)).astype(
        jnp.bfloat16
    )
    return (layer_out, new_state, new_conv)


def solution(mesh):
    placed = (
        P("ep", None),
        P(),
        P(None, "tp"),
        P(None, "tp"),
        P(None, "tp"),
        P(None, "tp"),
        P(),
        P("tp"),
        P("tp"),
        P(None, None, "tp"),
        P("ep", None, None, "tp"),
        P("ep", "tp", None, None),
        P("tp"),
        P("tp", None),
        P(),
        P(),
        P(),
        P(),
        P("ep", None),
        P("ep", None, "tp"),
        P("ep", None, "tp"),
        P("ep", "tp", None),
        P(),
        P("ep", "tp"),
        P("ep", "tp"),
        P("ep", "tp"),
        P("tp"),
    )
    return jax.shard_map(
        on_device,
        mesh=mesh,
        in_specs=placed,
        out_specs=(P("ep", "tp"), P("ep", "tp", None, None), P("ep", None, None, "tp")),
        check_vma=False,
    )
```

```python
import functools

import jax
import jax.numpy as jnp
from jax import lax
from jax.experimental import pallas as pl
from jax.experimental.pallas import tpu as pltpu
from jax.sharding import PartitionSpec as P

norm_eps = 1e-06


def scaled_rows(values, gain):
    values = values.astype(jnp.float32)
    mean_square = jnp.mean(values * values, axis=-1, keepdims=True)
    return values * lax.rsqrt(mean_square + norm_eps) * gain.astype(jnp.float32)


def softmax_plain(logits):
    weights = jnp.exp(logits)
    return weights / jnp.sum(weights, axis=-1, keepdims=True)


def fused_kernel(
    ep,
    group_size,
    group_count,
    expert_count,
    proj_out_ref,
    resid_ref,
    mix_ref,
    post_ref,
    ffn_ref,
    expert_router_ref,
    group_router_ref,
    switch_ref,
    route_ref,
    out_gain_ref,
    inner_ref,
    proj_step_ref,
    taps_ref,
    conv_ref,
    bias_ref,
    decay_ref,
    proj_x_hbm,
    proj_z_hbm,
    proj_b_hbm,
    proj_c_hbm,
    state_hbm,
    gate_hbm,
    up_hbm,
    down_hbm,
    dense_gate_hbm,
    dense_up_hbm,
    dense_down_hbm,
    out_ref,
    new_state_ref,
    new_conv_ref,
    proj_w,
    state_buf,
    keep_rows,
    vec_in_rows,
    router_buf,
    gate_w,
    up_w,
    down_w,
    dense_w,
    stream_buf,
    mix_own,
    mix_peer,
    half_own,
    half_far,
    rows_buf,
    aux_buf,
    part_buf,
    part_peer,
    send_x,
    recv_x,
    send_ep,
    recv_ep,
    square_own,
    square_peer,
    local_sem,
    dense_send,
    dense_recv,
    mix_send,
    mix_recv,
    rows_send,
    rows_recv,
    aux_send,
    aux_recv,
    part_send,
    part_recv,
    x_send,
    x_recv,
    ep_send,
    ep_recv,
    square_send,
    square_recv,
    entered,
    side_recv,
):
    f32, bf16 = jnp.float32, jnp.bfloat16
    me = lax.axis_index("ep")
    tp = lax.axis_index("tp")
    far = tp // 2
    core = tp % 2
    beside = far * 2 + (1 - core)
    across = (1 - far) * 2 + core
    diagonal = (1 - far) * 2 + (1 - core)
    near = (beside, across, diagonal)
    seqs, width = resid_ref.shape
    quarter = width // 4
    share = dense_w.shape[2]
    dgate, dup, ddown = dense_w.at[0], dense_w.at[1], dense_w.at[2]

    def remote(src, dst, send, recv, ep_to, tp_to):
        return pltpu.make_async_remote_copy(
            src_ref=src,
            dst_ref=dst,
            send_sem=send,
            recv_sem=recv,
            device_id=(ep_to, tp_to),
            device_id_type=pl.DeviceIdType.MESH,
        )

    def ep_at(step):
        return lax.rem(me + step + ep, ep)

    def load(src, dst, at):
        pltpu.make_async_copy(src, dst, local_sem.at[at]).start()

    def loaded(dst, at):
        pltpu.make_async_copy(dst, dst, local_sem.at[at]).wait()

    for k, src in enumerate((proj_x_hbm, proj_b_hbm, proj_c_hbm, proj_z_hbm)):
        load(src, proj_w.at[k], k)
    load(state_hbm, state_buf, 4)
    load(gate_hbm.at[0], gate_w, 5)
    load(up_hbm.at[0], up_w, 6)
    for q in range(4):
        load(down_hbm.at[0, :, pl.ds(q * quarter, quarter)], down_w.at[q], 7)
    dense_pairs = ((dense_gate_hbm, dgate), (dense_up_hbm, dup), (dense_down_hbm, ddown))
    for src, dst in dense_pairs:
        load(src.at[pl.ds(tp * share, share), :], dst.at[tp], 8)

    barrier = pltpu.get_barrier_semaphore()
    for step in range(1, ep):

        @pl.when(me + step < ep)
        def _():
            pl.semaphore_signal(
                barrier, inc=1, device_id=(ep_at(step), tp), device_id_type=pl.DeviceIdType.MESH
            )

    for peer in near:
        pl.semaphore_signal(
            barrier, inc=1, device_id=(me, peer), device_id_type=pl.DeviceIdType.MESH
        )

    def row(ref):
        return ref[...].astype(f32).reshape(1, ref.shape[0])

    resid_f = resid_ref[...].astype(f32)
    resid_scale = lax.rsqrt(jnp.mean(resid_f * resid_f, axis=1, keepdims=True) + norm_eps)
    normed = (resid_f * resid_scale * row(mix_ref)).astype(bf16)
    group_base = -(-expert_count // 8) * 8
    switch_lane = group_base + -(-group_count // 8) * 8
    router_buf[...] = jnp.zeros_like(router_buf)
    router_buf[0:expert_count, :] = expert_router_ref[...].astype(f32)
    router_buf[group_base : group_base + group_count, :] = group_router_ref[...].astype(f32)
    router_buf[switch_lane : switch_lane + 1, :] = row(switch_ref)
    nt = (((1,), (1,)), ((), ()))
    step_all = lax.dot_general(normed, proj_step_ref[...], nt, preferred_element_type=f32)
    pl.semaphore_wait(barrier, me + 3)
    for step in range(1, ep):

        @pl.when(me >= step)
        def _():
            pl.semaphore_signal(
                entered, inc=1, device_id=(me - step, tp), device_id_type=pl.DeviceIdType.MESH
            )


    sends = []

    def send_dense(t):
        src, dst = dense_pairs[t]
        for peer in near:
            remote(
                src.at[pl.ds(peer * share, share), :],
                dst.at[tp],
                dense_send,
                dense_recv,
                me,
                peer,
            ).start()

    send_dense(0)

    channels = conv_ref.shape[3]
    heads = bias_ref.shape[0]
    head_dim = channels // heads
    taps = taps_ref[...].astype(f32)
    old = conv_ref.shape[1]
    active = []
    for k in range(3):
        loaded(proj_w.at[k], k)
        fresh = jnp.dot(normed, proj_w[k], preferred_element_type=f32).astype(bf16)
        summed = conv_ref[k, 0].astype(f32) * taps[k, 0:1]
        for tap in range(1, old):
            earlier = conv_ref[k, tap]
            new_conv_ref[k, tap - 1] = earlier
            summed = summed + earlier.astype(f32) * taps[k, tap : tap + 1]
        new_conv_ref[k, old - 1] = fresh
        summed = summed + fresh.astype(f32) * taps[k, old : old + 1]
        active.append(summed * jax.nn.sigmoid(summed))
    inputs, vec_in, vec_read = active
    loaded(proj_w.at[3], 3)
    gate_z = jnp.dot(normed, proj_w[3], preferred_element_type=f32)
    step_lane = lax.broadcasted_iota(jnp.int32, step_all.shape, 1)
    lane_in = lax.broadcasted_iota(jnp.int32, (seqs, channels), 1)
    stepped = jnp.zeros((seqs, channels), f32)
    for h in range(heads):
        raw = jnp.sum(
            jnp.where(step_lane == tp * heads + h, step_all, 0.0), axis=1, keepdims=True
        )
        raw = raw + bias_ref[h]
        step = jnp.maximum(raw, 0.0) + jnp.log1p(jnp.exp(-jnp.abs(raw)))
        mine = (lane_in >= h * head_dim) & (lane_in < (h + 1) * head_dim)
        keep_rows[h] = jnp.broadcast_to(jnp.exp(-decay_ref[h] * step), (seqs, channels))
        stepped = jnp.where(mine, step, stepped)
    columns = jnp.concatenate(
        [stepped * inputs, jnp.zeros((channels - seqs, channels), f32)], axis=0
    ).T
    vec_in_rows[...] = vec_in
    read_rows = vec_read.astype(bf16)
    loaded(state_buf, 4)
    read_lane = lax.broadcasted_iota(jnp.int32, (head_dim, seqs), 1)
    reads = [jnp.zeros((head_dim, seqs), f32) for h in range(heads)]
    for t in range(seqs):
        for h in range(heads):
            part = pl.ds(h * head_dim, head_dim)
            fresh_state = (
                keep_rows[h, pl.ds(t, 1)] * state_buf[t, part]
                + columns[h * head_dim : (h + 1) * head_dim, t : t + 1]
                * vec_in_rows[pl.ds(t, 1)]
            )
            new_state_ref[t, part] = fresh_state
            value = lax.dot_general(
                fresh_state.astype(bf16), read_rows, nt, preferred_element_type=f32
            )
            reads[h] = jnp.where(read_lane == t, value, reads[h])
    read = jnp.concatenate(reads, axis=0)
    read = jnp.concatenate([read, jnp.zeros((channels, channels - seqs), f32)], axis=1)
    read = read.T[0:seqs]
    gated = (read * (gate_z * jax.nn.sigmoid(gate_z)) * row(inner_ref)).astype(bf16)
    mix_own[...] = jnp.dot(gated, proj_out_ref[...], preferred_element_type=f32).astype(bf16)

    first = remote(mix_own, mix_peer, mix_send.at[0], mix_recv.at[0], me, beside)
    first.start()
    sends.append(first)
    first.wait_recv()
    half = width // 2
    chip_sum = (mix_own[...].astype(f32) + mix_peer[...].astype(f32)).astype(bf16)
    half_own[0] = chip_sum[:, :half]
    half_own[1] = chip_sum[:, half:]
    over_x = remote(
        half_own.at[core], half_far.at[core], mix_send.at[1], mix_recv.at[1], me, across
    )
    over_x.start()
    send_dense(1)
    send_dense(2)

    over_x.wait_recv()
    to_core = remote(
        half_far.at[core], half_far.at[core], mix_send.at[2], mix_recv.at[2], me, beside
    )
    to_core.start()
    sends += [over_x, to_core]
    to_core.wait_recv()

    far_sum = jnp.concatenate([half_far[0], half_far[1]], axis=1)
    mixed = chip_sum.astype(f32) + far_sum.astype(f32)
    mixed_scale = lax.rsqrt(jnp.mean(mixed * mixed, axis=1, keepdims=True) + norm_eps)
    stream = (
        resid_f + mixed * mixed_scale * row(post_ref)
    ).astype(bf16)
    stream_f = stream.astype(f32)
    feed_scale = lax.rsqrt(jnp.mean(stream_f * stream_f, axis=1, keepdims=True) + norm_eps)
    feed_f = stream_f * feed_scale * row(ffn_ref)
    feed = feed_f.astype(bf16)
    my_z, my_y = me // 2, me % 2
    nz = ep // 2
    here = my_y * nz + my_z

    def feed_of(q):
        value = feed_f[:, :quarter]
        for other in range(1, 4):
            piece = feed_f[:, other * quarter : (other + 1) * quarter]
            value = jnp.where(q == other, piece, value)
        return value.astype(bf16)

    quarters = (tp, beside, across, diagonal)
    for k, q in enumerate(quarters):
        rows_buf[k, here] = feed_of(q)
    for q in range(4):
        stream_buf[q] = stream[:, q * quarter : (q + 1) * quarter]

    @pl.when(me + 1 < ep)
    def _():
        pl.semaphore_wait(entered, ep - 1 - me)

    def other(j):
        return j + (j - my_z + nz) // nz

    others = [other(j) for j in range(nz - 1)]
    upper = my_z // (nz // 2)
    far_first = [other(upper * j + (1 - upper) * (nz - 2 - j)) for j in range(nz - 1)]

    def rows_copy(k, at, ep_to, tp_to, k_to, side=None):
        return remote(
            rows_buf.at[k, at],
            rows_buf.at[k_to, at],
            rows_send,
            rows_recv.at[k_to // 2, at] if k_to % 2 == 0 else side_recv.at[side],
            ep_to,
            tp_to,
        )

    def aux_copy(at, ep_to):
        return remote(aux_buf.at[at], aux_buf.at[at], aux_send, aux_recv.at[at], ep_to, tp)

    def z_rows(z):
        return remote(
            rows_buf.at[0, here],
            rows_buf.at[0, here],
            rows_send,
            rows_recv.at[0, here],
            z * 2 + my_y,
            tp,
        )

    for z in far_first:
        z_rows(z).start()
    over_y = my_z * 2 + 1 - my_y
    rows_copy(0, here, over_y, tp, 0).start()
    rows_copy(2, here, over_y, tp, 2).start()

    logits = lax.dot_general(
        feed, router_buf[...].astype(bf16), nt, preferred_element_type=f32
    )
    lane = lax.broadcasted_iota(jnp.int32, logits.shape, 1)
    same = lax.broadcasted_iota(jnp.int32, (seqs, seqs), 0) == lax.broadcasted_iota(
        jnp.int32, (seqs, seqs), 1
    )
    route = lax.dot_general(
        jnp.where(same, 1.0, 0.0).astype(bf16),
        route_ref[...].astype(f32).astype(bf16),
        nt,
        preferred_element_type=f32,
    ).astype(jnp.int32)
    picked = lane == route[:, 0:1]
    for k in range(1, route.shape[1]):
        picked = picked | (lane == route[:, k : k + 1])
    weights = jnp.exp(logits)
    pick = jnp.where(picked, weights, 0.0)
    group_lane = (lane - group_base) * group_size
    in_groups = (lane >= group_base) & (lane < group_base + group_count)
    group = jnp.where(in_groups, weights, 0.0)
    lead = route[:, 0:1]
    chosen = in_groups & (lead >= group_lane) & (lead < group_lane + group_size)
    group_weight = jnp.sum(jnp.where(chosen, weights, 0.0), axis=1, keepdims=True) / jnp.sum(
        group, axis=1, keepdims=True
    )
    pick = pick / jnp.sum(pick, axis=1, keepdims=True) * group_weight
    aux_buf[here] = jnp.where(lane == switch_lane, jax.nn.sigmoid(logits), pick).astype(bf16)
    for z in far_first:
        aux_copy(here, z * 2 + my_y).start()
    aux_copy(here, over_y).start()

    total = nz * seqs
    sides = (my_y, 1 - my_y)

    def at_of(side, z):
        return sides[side] * nz + z

    def arrived(k, at):
        rows_copy(k, at, me, beside, k).wait_recv()

    there = at_of(1, my_z)
    for z in others:
        at = at_of(0, z)
        arrived(0, at)
        rows_copy(0, at, over_y, tp, 0).start()
        rows_copy(0, at, me, across, 2).start()
        rows_copy(0, at, me, beside, 1, 0).start()
    arrived(0, there)
    rows_copy(0, there, me, beside, 1, 1).start()
    arrived(2, there)
    rows_copy(2, there, me, beside, 3, 1).start()
    for z in others:
        at = at_of(0, z)
        aux_copy(at, me).wait_recv()
        aux_copy(at, over_y).start()
    for z in others:
        at = at_of(1, z)
        arrived(0, at)
        rows_copy(0, at, me, across, 2).start()
        rows_copy(0, at, me, beside, 1, 1).start()
    for z in others:
        at = at_of(0, z)
        arrived(2, at)
        rows_copy(2, at, me, beside, 3, 0).start()

    def gather_end(side):
        for z in range(nz) if side else others:
            at = at_of(side, z)
            if side:
                aux_copy(at, me).wait_recv()
        blocks = rows_buf.at[0:2, 0 : nz if side else nz - 1]
        remote(blocks, blocks, rows_send, side_recv.at[side], me, beside).wait_recv()

    def add(total_sum, value):
        return value if total_sum is None else total_sum + value

    def part_copy(k, side):
        block = pl.ds(sides[side] * nz, nz)
        return remote(
            part_buf.at[(diagonal, beside)[k], block],
            part_peer.at[k, block],
            part_send,
            part_recv.at[k, side],
            me,
            beside,
        )

    def feed_forward(side):
        block = pl.ds(sides[side] * nz, nz)
        gate = up = dense_g = dense_u = None
        for k, q in enumerate(quarters):
            rows = rows_buf[k, block].reshape(total, quarter)
            span = pl.ds(pl.multiple_of(q * quarter, quarter), quarter)
            gate = add(gate, jnp.dot(rows, gate_w[span, :], preferred_element_type=f32))
            up = add(up, jnp.dot(rows, up_w[span, :], preferred_element_type=f32))
            dense_g = add(
                dense_g, lax.dot_general(rows, dgate[q], nt, preferred_element_type=f32)
            )
            dense_u = add(dense_u, lax.dot_general(rows, dup[q], nt, preferred_element_type=f32))
        aux = aux_buf[block].reshape(total, aux_buf.shape[2]).astype(f32)
        aux_lane = lax.broadcasted_iota(jnp.int32, aux.shape, 1)
        weight = jnp.sum(jnp.where(aux_lane == me, aux, 0.0), axis=1, keepdims=True)
        switch = jnp.sum(jnp.where(aux_lane == switch_lane, aux, 0.0), axis=1, keepdims=True)
        hidden = (gate * jax.nn.sigmoid(gate) * up * weight).astype(bf16)
        dense_hidden = (dense_g * jax.nn.sigmoid(dense_g) * dense_u * switch).astype(bf16)
        for k, q in enumerate((diagonal, beside, across, tp)):
            value = jnp.dot(hidden, down_w[q], preferred_element_type=f32) + jnp.dot(
                dense_hidden, ddown[q], preferred_element_type=f32
            )
            part_buf[q, block] = value.astype(bf16).reshape(nz, seqs, quarter)
            if k < 2:
                part_copy(k, side).start()

    far_then_own = far_first + [my_z]

    def x_copy(at):
        return remote(send_x.at[at], recv_x.at[at], x_send, x_recv.at[at], me, across)

    def sums_over_x(side):
        part_copy(0, side).wait_recv()
        for z in far_then_own:
            at = at_of(side, z)
            send_x[at] = (
                part_buf[across, at].astype(f32) + part_peer[0, at].astype(f32)
            ).astype(bf16)
            x_copy(at).start()

    def ep_copy(at, slot, ep_to):
        return remote(
            send_ep.at[at], recv_ep.at[slot], ep_send, ep_recv, ep_to, tp
        )

    def summed(at):
        x_copy(at).wait_recv()
        return (
            part_buf[tp, at].astype(f32)
            + part_peer[1, at].astype(f32)
            + recv_x[at].astype(f32)
        )

    def sums_over_ep(side):
        part_copy(1, side).wait_recv()
        for z in far_then_own if side else far_first:
            at = at_of(side, z)
            send_ep[at] = summed(at).astype(bf16)
            ep_copy(at, here, z * 2 + sides[side]).start()

    loaded(gate_w, 5)
    loaded(up_w, 6)
    loaded(down_w, 7)
    loaded(dense_w.at[:, tp], 8)
    others_dense = dense_w.at[:, 0:3]
    all_dense = remote(others_dense, others_dense, dense_send, dense_recv, me, beside)
    all_dense.wait_recv()
    gather_end(0)
    feed_forward(0)
    for z in others:
        at = at_of(1, z)
        arrived(2, at)
        rows_copy(2, at, me, beside, 3, 1).start()
    sums_over_x(0)
    gather_end(1)
    feed_forward(1)
    sums_over_ep(0)
    sums_over_x(1)
    combined = summed(here)
    sums_over_ep(1)

    seven = pl.ds(0, ep - 1)
    remote(send_ep.at[seven], recv_ep.at[seven], ep_send, ep_recv, me, beside).wait_recv()
    for side in range(2):
        for z in range(nz) if side else others:
            combined = combined + recv_ep[at_of(side, z)].astype(f32)

    square = jnp.sum(combined * combined, axis=1, keepdims=True)
    lanes = square_own.shape[1]
    row_id = lax.broadcasted_iota(jnp.int32, (seqs, lanes), 0)
    diagonal_lane = row_id == lax.broadcasted_iota(jnp.int32, (seqs, lanes), 1)
    square_row = jnp.sum(jnp.where(diagonal_lane, square, 0.0), axis=0, keepdims=True)
    square_own[...] = jnp.broadcast_to(square_row, square_own.shape)
    for k, peer in enumerate(near):
        remote(square_own, square_peer.at[k], square_send, square_recv, me, peer).start()
    all_squares = remote(square_peer, square_peer, square_send, square_recv, me, beside)
    all_squares.wait_recv()
    everything = (square_own[...] + square_peer[0]) + (square_peer[1] + square_peer[2])
    spread = jnp.where(diagonal_lane, everything[0:1], 0.0)
    scale = lax.rsqrt(jnp.sum(spread, axis=1, keepdims=True) / width + norm_eps)
    own_stream = stream_buf[tp].astype(f32)
    out_ref[...] = (own_stream + combined * scale * row(out_gain_ref)).astype(bf16)
    for copy in sends:
        copy.wait_send()
    blocks = rows_buf.at[:, seven]
    for ref, sem in (
        (blocks, rows_send),
        (aux_buf.at[seven], aux_send),
        (part_peer, part_send),
        (send_x, x_send),
        (send_ep.at[seven], ep_send),
    ):
        remote(ref, ref, sem, mix_recv.at[0], me, beside).wait_send()
    all_dense.wait_send()
    all_squares.wait_send()


def write_kernel(out_ref, state_ref, conv_ref, out_hbm, state_hbm, conv_hbm, sems):
    pairs = ((state_ref, state_hbm), (conv_ref, conv_hbm), (out_ref, out_hbm))
    copies = [pltpu.make_async_copy(src, dst, sems.at[k]) for k, (src, dst) in enumerate(pairs)]
    for copy in copies:
        copy.start()
    for copy in copies:
        copy.wait()


def fused_layer(
    resid,
    mix_gain,
    proj_x,
    proj_z,
    proj_b,
    proj_c,
    proj_step,
    step_bias,
    decay_rate,
    conv_taps,
    conv_state,
    scan_state,
    inner_gain,
    proj_out,
    post_gain,
    ffn_gain,
    group_router,
    expert_router,
    route_experts,
    expert_gate,
    expert_up,
    expert_down,
    dense_switch,
    dense_gate,
    dense_up,
    dense_down,
    out_gain,
):
    ep = lax.axis_size("ep")
    seqs, width = resid.shape
    quarter = width // 4
    channels = conv_state.shape[3]
    expert_count = expert_router.shape[1]
    group_count = group_router.shape[1]
    lanes = 128
    hidden_here = expert_gate.shape[2]
    share = dense_gate.shape[0] // 4
    bf16 = jnp.bfloat16
    vmem = pl.BlockSpec(memory_space=pltpu.VMEM)
    hbm = pl.BlockSpec(memory_space=pl.ANY)
    dma = pltpu.SemaphoreType.DMA
    kernel = functools.partial(
        fused_kernel, ep, expert_count // group_count, group_count, expert_count
    )
    smem = pl.BlockSpec(memory_space=pltpu.SMEM)
    earlier = conv_state.transpose(1, 2, 0, 3)
    state = scan_state.reshape(seqs, channels, scan_state.shape[3])
    results = pl.pallas_call(
        kernel,
        out_shape=(
            pltpu.VMEM((seqs, quarter), bf16),
            pltpu.VMEM(state.shape, state.dtype),
            pltpu.VMEM(earlier.shape, earlier.dtype),
        ),
        in_specs=[vmem] * 14 + [smem] * 2 + [hbm] * 11,
        out_specs=(vmem, vmem, vmem),
        scratch_shapes=[
            pltpu.VMEM((4,) + proj_x.shape, bf16),
            pltpu.VMEM(state.shape, state.dtype),
            pltpu.VMEM((step_bias.shape[0], seqs, channels), jnp.float32),
            pltpu.VMEM((seqs, channels), jnp.float32),
            pltpu.VMEM((lanes, width), jnp.float32),
            pltpu.VMEM((width, hidden_here), bf16),
            pltpu.VMEM((width, hidden_here), bf16),
            pltpu.VMEM((4, hidden_here, quarter), bf16),
            pltpu.VMEM((3, 4, share, quarter), bf16),
            pltpu.VMEM((4, seqs, quarter), bf16),
            pltpu.VMEM((seqs, width), bf16),
            pltpu.VMEM((seqs, width), bf16),
            pltpu.VMEM((2, seqs, width // 2), bf16),
            pltpu.VMEM((2, seqs, width // 2), bf16),
            pltpu.VMEM((4, ep, seqs, quarter), bf16),
            pltpu.VMEM((ep, seqs, lanes), bf16),
            pltpu.VMEM((4, ep, seqs, quarter), bf16),
            pltpu.VMEM((2, ep, seqs, quarter), bf16),
            pltpu.VMEM((ep, seqs, quarter), bf16),
            pltpu.VMEM((ep, seqs, quarter), bf16),
            pltpu.VMEM((ep, seqs, quarter), bf16),
            pltpu.VMEM((ep, seqs, quarter), bf16),
            pltpu.VMEM((8, lanes), jnp.float32),
            pltpu.VMEM((3, 8, lanes), jnp.float32),
            dma((9,)),
            dma,
            dma,
            dma((3,)),
            dma((3,)),
            dma,
            dma((2, ep)),
            dma,
            dma((ep,)),
            dma,
            dma((2, 2)),
            dma,
            dma((ep,)),
            dma,
            dma,
            dma,
            dma,
            pltpu.SemaphoreType.REGULAR,
            dma((2,)),
        ],
        compiler_params=pltpu.CompilerParams(collective_id=0, has_side_effects=True),
        name="fused_layer",
    )(
        proj_out,
        resid,
        mix_gain,
        post_gain,
        ffn_gain,
        expert_router.T,
        group_router.T,
        dense_switch,
        route_experts.T,
        out_gain,
        inner_gain,
        proj_step.T,
        conv_taps,
        earlier,
        step_bias,
        decay_rate,
        proj_x,
        proj_z,
        proj_b,
        proj_c,
        state,
        expert_gate,
        expert_up,
        expert_down,
        dense_gate,
        dense_up,
        dense_down,
    )
    layer_out, new_state, new_conv = pl.pallas_call(
        write_kernel,
        out_shape=tuple(jax.ShapeDtypeStruct(one.shape, one.dtype) for one in results),
        in_specs=[vmem] * 3,
        out_specs=(hbm, hbm, hbm),
        scratch_shapes=[dma((3,))],
        compiler_params=pltpu.CompilerParams(vmem_limit_bytes=4 << 20),
        name="write_results",
    )(*results)
    return layer_out, new_state.reshape(scan_state.shape), new_conv.transpose(2, 0, 1, 3)


def on_device(
    resid,
    mix_gain,
    proj_x,
    proj_z,
    proj_b,
    proj_c,
    proj_step,
    step_bias,
    decay_rate,
    conv_taps,
    conv_state,
    scan_state,
    inner_gain,
    proj_out,
    post_gain,
    ffn_gain,
    group_router,
    expert_router,
    route_experts,
    expert_gate,
    expert_up,
    expert_down,
    dense_switch,
    dense_gate,
    dense_up,
    dense_down,
    out_gain,
):
    tp_index = lax.axis_index("tp")
    seqs = resid.shape[0]
    width = resid.shape[1]
    quarter = width // lax.axis_size("tp")
    heads_here = scan_state.shape[1]
    head_dim = scan_state.shape[2]
    state_dim = scan_state.shape[3]
    channels = conv_state.shape[3]
    repeat = heads_here // (channels // state_dim)
    whole_blocks = 2 * seqs * route_experts.shape[1] // expert_router.shape[1] >= seqs
    one_group = channels == state_dim == 128 and expert_router.shape[1] <= 64
    few = lax.axis_size("tp") == 4 and expert_gate.shape[0] == 1
    few = few and lax.axis_size("ep") % 2 == 0
    if whole_blocks and one_group and few:
        return fused_layer(
            resid,
            mix_gain,
            proj_x,
            proj_z,
            proj_b,
            proj_c,
            proj_step,
            step_bias,
            decay_rate,
            conv_taps,
            conv_state,
            scan_state,
            inner_gain,
            proj_out,
            post_gain,
            ffn_gain,
            group_router,
            expert_router,
            route_experts,
            expert_gate,
            expert_up,
            expert_down,
            dense_switch,
            dense_gate,
            dense_up,
            dense_down,
            out_gain,
        )
    normed = scaled_rows(resid, mix_gain).astype(jnp.bfloat16)
    fresh = jnp.stack(
        [
            jnp.dot(normed, proj_x, preferred_element_type=jnp.float32),
            jnp.dot(normed, proj_b, preferred_element_type=jnp.float32),
            jnp.dot(normed, proj_c, preferred_element_type=jnp.float32),
        ],
        axis=1,
    ).astype(jnp.bfloat16)
    gate_z = jnp.dot(normed, proj_z, preferred_element_type=jnp.float32)
    step_all = jnp.dot(normed, proj_step, preferred_element_type=jnp.float32)
    step_raw = lax.dynamic_slice_in_dim(step_all, tp_index * heads_here, heads_here, 1)
    history = jnp.concatenate([conv_state, fresh[:, :, None, :]], axis=2)
    activated = jax.nn.silu(
        jnp.sum(history.astype(jnp.float32) * conv_taps.astype(jnp.float32)[None], axis=2)
    )
    xs_heads = activated[:, 0].reshape(seqs, heads_here, head_dim)
    b_heads = jnp.repeat(activated[:, 1].reshape(seqs, -1, state_dim), repeat, axis=1)
    c_heads = jnp.repeat(activated[:, 2].reshape(seqs, -1, state_dim), repeat, axis=1)
    step = jax.nn.softplus(step_raw + step_bias)
    keep = jnp.exp(-decay_rate * step)
    driven = step[:, :, None] * xs_heads
    new_state = keep[:, :, None, None] * scan_state + driven[:, :, :, None] * b_heads[:, :, None, :]
    read = jnp.sum(new_state * c_heads[:, :, None, :], axis=3).reshape(seqs, channels)
    gated = (read * jax.nn.silu(gate_z) * inner_gain.astype(jnp.float32)).astype(jnp.bfloat16)
    new_conv = history[:, :, 1:, :]
    mixed = lax.psum(
        jnp.dot(gated, proj_out, preferred_element_type=jnp.float32).astype(jnp.bfloat16), "tp"
    ).astype(jnp.float32)
    stream = (resid.astype(jnp.float32) + scaled_rows(mixed, post_gain)).astype(jnp.bfloat16)
    feed = scaled_rows(stream, ffn_gain).astype(jnp.bfloat16)
    feed_quarter = lax.dynamic_slice_in_dim(feed, tp_index * quarter, quarter, 1)
    expert_count = expert_router.shape[1]
    group_size = expert_count // group_router.shape[1]
    pick_count = route_experts.shape[1]
    group_prob = softmax_plain(jnp.dot(feed, group_router, preferred_element_type=jnp.float32))
    expert_logits = jnp.dot(feed, expert_router, preferred_element_type=jnp.float32)
    matches = route_experts[:, :, None] == jnp.arange(expert_count, dtype=jnp.int32)[None, None, :]
    pick_logits = jnp.sum(jnp.where(matches, expert_logits[:, None, :], 0.0), axis=2)
    chosen_group = route_experts[:, 0] // group_size
    group_ids = jnp.arange(group_router.shape[1], dtype=jnp.int32)
    group_weight = jnp.sum(
        jnp.where(chosen_group[:, None] == group_ids[None, :], group_prob, 0.0), axis=1
    )
    pick_weight = softmax_plain(pick_logits) * group_weight[:, None]
    capacity = 2 * seqs * pick_count // expert_count
    flat_picks = route_experts.reshape(-1)
    one_hot = (flat_picks[:, None] == jnp.arange(expert_count, dtype=jnp.int32)[None, :]).astype(
        jnp.int32
    )
    slot = jnp.sum((jnp.cumsum(one_hot, axis=0) - one_hot) * one_hot, axis=1)
    target = flat_picks * capacity + slot
    repeated = jnp.repeat(feed, pick_count, axis=0)
    outgoing = jnp.zeros((expert_count * capacity, width), jnp.bfloat16).at[target].set(repeated)
    outgoing = outgoing.reshape(expert_count, capacity, width)
    arrived = lax.all_to_all(outgoing, "ep", split_axis=0, concat_axis=0, tiled=True)
    sources = arrived.shape[0]
    items = arrived.shape[1]
    rows = arrived.reshape(sources * items, width)
    gate_value = jnp.dot(rows, expert_gate[0], preferred_element_type=jnp.float32)
    up_value = jnp.dot(rows, expert_up[0], preferred_element_type=jnp.float32)
    hidden = (jax.nn.silu(gate_value) * up_value).astype(jnp.bfloat16)
    result = jnp.dot(hidden, expert_down[0], preferred_element_type=jnp.float32).reshape(
        sources, items, width
    )
    summed = lax.psum_scatter(result.astype(jnp.bfloat16), "tp", scatter_dimension=2, tiled=True)
    returned = lax.all_to_all(summed, "ep", split_axis=0, concat_axis=0, tiled=True)
    fetched = returned.reshape(expert_count * capacity, quarter)[target].reshape(
        seqs, pick_count, quarter
    )
    routed = jnp.sum(fetched.astype(jnp.float32) * pick_weight[:, :, None], axis=1)
    gate_piece = jnp.einsum(
        "sd,cd->sc",
        feed_quarter,
        lax.all_gather(dense_gate, "ep", axis=0, tiled=True),
        preferred_element_type=jnp.float32,
    )
    up_piece = jnp.einsum(
        "sd,cd->sc",
        feed_quarter,
        lax.all_gather(dense_up, "ep", axis=0, tiled=True),
        preferred_element_type=jnp.float32,
    )
    gate_sum = gate_piece
    up_sum = up_piece
    gate_sum, up_sum = (
        lax.psum(gate_sum.astype(jnp.bfloat16), "tp").astype(jnp.float32),
        lax.psum(up_sum.astype(jnp.bfloat16), "tp").astype(jnp.float32),
    )
    dense_hidden = (jax.nn.silu(gate_sum) * up_sum).astype(jnp.bfloat16)
    dense_out = jnp.dot(
        dense_hidden,
        lax.all_gather(dense_down, "ep", axis=0, tiled=True),
        preferred_element_type=jnp.float32,
    )
    switch = jax.nn.sigmoid(jnp.dot(feed, dense_switch, preferred_element_type=jnp.float32))
    combined = routed + switch[:, None] * dense_out
    total_square = lax.psum(jnp.sum(combined * combined, axis=1), "tp")
    scale = lax.rsqrt(total_square / width + norm_eps)
    stream_part = lax.dynamic_slice_in_dim(stream, tp_index * quarter, quarter, 1).astype(
        jnp.float32
    )
    layer_out = (stream_part + combined * scale[:, None] * out_gain.astype(jnp.float32)).astype(
        jnp.bfloat16
    )
    return (layer_out, new_state, new_conv)


def solution(mesh):
    placed = (
        P("ep", None),
        P(),
        P(None, "tp"),
        P(None, "tp"),
        P(None, "tp"),
        P(None, "tp"),
        P(),
        P("tp"),
        P("tp"),
        P(None, None, "tp"),
        P("ep", None, None, "tp"),
        P("ep", "tp", None, None),
        P("tp"),
        P("tp", None),
        P(),
        P(),
        P(),
        P(),
        P("ep", None),
        P("ep", None, "tp"),
        P("ep", None, "tp"),
        P("ep", "tp", None),
        P(),
        P("ep", "tp"),
        P("ep", "tp"),
        P("ep", "tp"),
        P("tp"),
    )
    return jax.shard_map(
        on_device,
        mesh=mesh,
        in_specs=placed,
        out_specs=(P("ep", "tp"), P("ep", "tp", None, None), P("ep", None, None, "tp")),
        check_vma=False,
    )
```

```python
import functools

import jax
import jax.numpy as jnp
from jax import lax
from jax.experimental import pallas as pl
from jax.experimental.pallas import tpu as pltpu
from jax.sharding import PartitionSpec as P

norm_eps = 1e-06


def scaled_rows(values, gain):
    values = values.astype(jnp.float32)
    mean_square = jnp.mean(values * values, axis=-1, keepdims=True)
    return values * lax.rsqrt(mean_square + norm_eps) * gain.astype(jnp.float32)


def softmax_plain(logits):
    weights = jnp.exp(logits)
    return weights / jnp.sum(weights, axis=-1, keepdims=True)


def fused_kernel(
    ep,
    group_size,
    group_count,
    expert_count,
    proj_out_hbm,
    resid_hbm,
    mix_hbm,
    post_hbm,
    ffn_hbm,
    expert_router_hbm,
    group_router_hbm,
    switch_hbm,
    route_hbm,
    out_gain_hbm,
    inner_hbm,
    proj_step_hbm,
    taps_hbm,
    conv_hbm,
    bias_hbm,
    decay_hbm,
    proj_x_hbm,
    proj_z_hbm,
    proj_b_hbm,
    proj_c_hbm,
    state_hbm,
    gate_hbm,
    up_hbm,
    down_hbm,
    dense_gate_hbm,
    dense_up_hbm,
    dense_down_hbm,
    out_ref,
    new_state_ref,
    new_conv_ref,
    proj_w,
    state_buf,
    keep_rows,
    vec_in_rows,
    router_buf,
    gate_w,
    up_w,
    down_w,
    dense_w,
    stream_buf,
    mix_own,
    mix_peer,
    half_own,
    half_far,
    rows_buf,
    aux_buf,
    part_buf,
    part_peer,
    send_x,
    recv_x,
    send_ep,
    recv_ep,
    square_own,
    square_peer,
    local_sem,
    dense_send,
    dense_recv,
    mix_send,
    mix_recv,
    rows_send,
    rows_recv,
    aux_send,
    aux_recv,
    part_send,
    part_recv,
    x_send,
    x_recv,
    ep_send,
    ep_recv,
    square_send,
    square_recv,
    entered,
    side_recv,
    small_sem,
    proj_out_ref,
    resid_ref,
    mix_ref,
    post_ref,
    ffn_ref,
    expert_router_ref,
    group_router_ref,
    switch_ref,
    route_ref,
    out_gain_ref,
    inner_ref,
    proj_step_ref,
    taps_ref,
    conv_ref,
    bias_ref,
    decay_ref,
):
    f32, bf16 = jnp.float32, jnp.bfloat16
    me = lax.axis_index("ep")
    tp = lax.axis_index("tp")
    far = tp // 2
    core = tp % 2
    beside = far * 2 + (1 - core)
    across = (1 - far) * 2 + core
    diagonal = (1 - far) * 2 + (1 - core)
    near = (beside, across, diagonal)
    seqs, width = resid_ref.shape
    quarter = width // 4
    share = dense_w.shape[1]
    dense_at = (tp * 2, tp * 2 + 1, tp + 8)

    def remote(src, dst, send, recv, ep_to, tp_to):
        return pltpu.make_async_remote_copy(
            src_ref=src,
            dst_ref=dst,
            send_sem=send,
            recv_sem=recv,
            device_id=(ep_to, tp_to),
            device_id_type=pl.DeviceIdType.MESH,
        )

    def ep_at(step):
        return lax.rem(me + step + ep, ep)

    barrier = pltpu.get_barrier_semaphore()
    for step in range(1, ep):

        @pl.when(me + step < ep)
        def _():
            pl.semaphore_signal(
                barrier, inc=1, device_id=(ep_at(step), tp), device_id_type=pl.DeviceIdType.MESH
            )

    for peer in near:
        pl.semaphore_signal(
            barrier, inc=1, device_id=(me, peer), device_id_type=pl.DeviceIdType.MESH
        )

    def load(src, dst, at):
        pltpu.make_async_copy(src, dst, local_sem.at[at]).start()

    def loaded(dst, at):
        pltpu.make_async_copy(dst, dst, local_sem.at[at]).wait()

    small_pairs = (
        (resid_hbm, resid_ref),
        (mix_hbm, mix_ref),
        (proj_step_hbm, proj_step_ref),
        (taps_hbm, taps_ref),
        (conv_hbm, conv_ref),
        (bias_hbm, bias_ref),
        (decay_hbm, decay_ref),
        (inner_hbm, inner_ref),
        (proj_out_hbm, proj_out_ref),
        (post_hbm, post_ref),
        (ffn_hbm, ffn_ref),
        (expert_router_hbm, expert_router_ref),
        (group_router_hbm, group_router_ref),
        (switch_hbm, switch_ref),
        (route_hbm, route_ref),
        (out_gain_hbm, out_gain_ref),
    )
    small_copies = [
        pltpu.make_async_copy(src, dst, small_sem.at[k])
        for k, (src, dst) in enumerate(small_pairs)
    ]
    for copy in small_copies[:5]:
        copy.start()
    for k, src in enumerate((proj_x_hbm, proj_b_hbm, proj_c_hbm, proj_z_hbm)):
        load(src, proj_w.at[k], k)
    load(state_hbm, state_buf, 4)
    for copy in small_copies[5:]:
        copy.start()
    dense_srcs = (dense_gate_hbm, dense_up_hbm, dense_down_hbm)

    def row(ref):
        return ref[...].astype(f32).reshape(1, ref.shape[0])

    pl.semaphore_wait(barrier, me + 3)
    for step in range(1, ep):

        @pl.when(me >= step)
        def _():
            pl.semaphore_signal(
                entered, inc=1, device_id=(me - step, tp), device_id_type=pl.DeviceIdType.MESH
            )


    sends = []

    def send_dense(t):
        src, dst = dense_srcs[t], dense_w.at[dense_at[t]]
        for peer in near:
            remote(
                src.at[pl.ds(peer * share, share), :],
                dst,
                dense_send,
                dense_recv,
                me,
                peer,
            ).start()

    send_dense(0)

    @pl.when(core == 0)
    def _():
        send_dense(1)


    for copy in small_copies[:3]:
        copy.wait()
    resid_f = resid_ref[...].astype(f32)
    resid_scale = lax.rsqrt(jnp.mean(resid_f * resid_f, axis=1, keepdims=True) + norm_eps)
    normed = (resid_f * resid_scale * row(mix_ref)).astype(bf16)
    group_base = -(-expert_count // 8) * 8
    switch_lane = group_base + -(-group_count // 8) * 8
    nt = (((1,), (1,)), ((), ()))
    step_all = lax.dot_general(normed, proj_step_ref[...], nt, preferred_element_type=f32)
    channels = conv_ref.shape[3]
    heads = bias_ref.shape[0]
    head_dim = channels // heads
    for copy in small_copies[3:7]:
        copy.wait()
    taps = taps_ref[...].astype(f32)
    old = conv_ref.shape[1]
    active = []
    for k in range(3):
        loaded(proj_w.at[k], k)
        fresh = jnp.dot(normed, proj_w[k], preferred_element_type=f32).astype(bf16)
        summed = conv_ref[k, 0].astype(f32) * taps[k, 0:1]
        for tap in range(1, old):
            earlier = conv_ref[k, tap]
            new_conv_ref[k, tap - 1] = earlier
            summed = summed + earlier.astype(f32) * taps[k, tap : tap + 1]
        new_conv_ref[k, old - 1] = fresh
        summed = summed + fresh.astype(f32) * taps[k, old : old + 1]
        active.append(summed * jax.nn.sigmoid(summed))
    inputs, vec_in, vec_read = active
    loaded(proj_w.at[3], 3)
    gate_z = jnp.dot(normed, proj_w[3], preferred_element_type=f32)
    step_lane = lax.broadcasted_iota(jnp.int32, step_all.shape, 1)
    lane_in = lax.broadcasted_iota(jnp.int32, (seqs, channels), 1)
    stepped = jnp.zeros((seqs, channels), f32)
    for h in range(heads):
        raw = jnp.sum(
            jnp.where(step_lane == tp * heads + h, step_all, 0.0), axis=1, keepdims=True
        )
        raw = raw + bias_ref[h]
        step = jnp.maximum(raw, 0.0) + jnp.log1p(jnp.exp(-jnp.abs(raw)))
        mine = (lane_in >= h * head_dim) & (lane_in < (h + 1) * head_dim)
        keep_rows[h] = jnp.broadcast_to(jnp.exp(-decay_ref[h] * step), (seqs, channels))
        stepped = jnp.where(mine, step, stepped)
    columns = jnp.concatenate(
        [stepped * inputs, jnp.zeros((channels - seqs, channels), f32)], axis=0
    ).T
    vec_in_rows[...] = vec_in
    read_rows = vec_read.astype(bf16)
    for copy in small_copies[7:]:
        copy.wait()
    loaded(state_buf, 4)
    load(gate_hbm.at[0], gate_w, 5)
    load(up_hbm.at[0], up_w, 6)
    for q in range(4):
        load(down_hbm.at[0, :, pl.ds(q * quarter, quarter)], down_w.at[q], 7)
    for src, at in zip(dense_srcs, dense_at):
        load(src.at[pl.ds(tp * share, share), :], dense_w.at[at], 8)
    read_lane = lax.broadcasted_iota(jnp.int32, (head_dim, seqs), 1)
    reads = [jnp.zeros((head_dim, seqs), f32) for h in range(heads)]
    for t in range(seqs):
        for h in range(heads):
            part = pl.ds(h * head_dim, head_dim)
            fresh_state = (
                keep_rows[h, pl.ds(t, 1)] * state_buf[t, part]
                + columns[h * head_dim : (h + 1) * head_dim, t : t + 1]
                * vec_in_rows[pl.ds(t, 1)]
            )
            new_state_ref[t, part] = fresh_state
            value = lax.dot_general(
                fresh_state.astype(bf16), read_rows, nt, preferred_element_type=f32
            )
            reads[h] = jnp.where(read_lane == t, value, reads[h])
    read = jnp.concatenate(reads, axis=0)
    read = jnp.concatenate([read, jnp.zeros((channels, channels - seqs), f32)], axis=1)
    read = read.T[0:seqs]
    gated = (read * (gate_z * jax.nn.sigmoid(gate_z)) * row(inner_ref)).astype(bf16)
    mix_own[...] = jnp.dot(gated, proj_out_ref[...], preferred_element_type=f32).astype(bf16)

    first = remote(mix_own, mix_peer, mix_send.at[0], mix_recv.at[0], me, beside)
    first.start()
    sends.append(first)
    first.wait_recv()
    half = width // 2
    chip_sum = (mix_own[...].astype(f32) + mix_peer[...].astype(f32)).astype(bf16)
    half_own[0] = chip_sum[:, :half]
    half_own[1] = chip_sum[:, half:]

    def far_half(h, tp_to, src):
        return remote(src.at[h], half_far.at[h], mix_send.at[1], mix_recv.at[1 + h], me, tp_to)

    @pl.when(core == 1)
    def _():
        for h in range(2):
            far_half(h, across, half_own).start()
        send_dense(1)
        send_dense(2)

    router_buf[...] = jnp.zeros_like(router_buf)
    router_buf[0:expert_count, :] = expert_router_ref[...].astype(f32)
    router_buf[group_base : group_base + group_count, :] = group_router_ref[...].astype(f32)
    router_buf[switch_lane : switch_lane + 1, :] = row(switch_ref)

    for h in range(2):
        far_half(h, across, half_own).wait_recv()

        @pl.when(core == 1)
        def _():
            far_half(h, beside, half_far).start()

    @pl.when(core == 0)
    def _():
        send_dense(2)

    far_sum = jnp.concatenate([half_far[0], half_far[1]], axis=1)
    mixed = chip_sum.astype(f32) + far_sum.astype(f32)
    mixed_scale = lax.rsqrt(jnp.mean(mixed * mixed, axis=1, keepdims=True) + norm_eps)
    stream = (
        resid_f + mixed * mixed_scale * row(post_ref)
    ).astype(bf16)
    stream_f = stream.astype(f32)
    feed_scale = lax.rsqrt(jnp.mean(stream_f * stream_f, axis=1, keepdims=True) + norm_eps)
    feed_f = stream_f * feed_scale * row(ffn_ref)
    feed = feed_f.astype(bf16)
    my_z, my_y = me // 2, me % 2
    nz = ep // 2
    here = my_y * nz + my_z

    def feed_of(q):
        value = feed_f[:, :quarter]
        for other in range(1, 4):
            piece = feed_f[:, other * quarter : (other + 1) * quarter]
            value = jnp.where(q == other, piece, value)
        return value.astype(bf16)

    quarters = (tp, beside, across, diagonal)
    for k, q in enumerate(quarters):
        rows_buf[k, here] = feed_of(q)
    for q in range(4):
        stream_buf[q] = stream[:, q * quarter : (q + 1) * quarter]

    @pl.when(me + 1 < ep)
    def _():
        pl.semaphore_wait(entered, ep - 1 - me)

    def other(j):
        return j + (j - my_z + nz) // nz

    others = [other(j) for j in range(nz - 1)]
    upper = my_z // (nz // 2)
    far_first = [other(upper * j + (1 - upper) * (nz - 2 - j)) for j in range(nz - 1)]

    def rows_copy(k, at, ep_to, tp_to, k_to, side=None):
        return remote(
            rows_buf.at[k, at],
            rows_buf.at[k_to, at],
            rows_send,
            rows_recv.at[k_to // 2, at] if k_to % 2 == 0 else side_recv.at[side],
            ep_to,
            tp_to,
        )

    def aux_copy(side, ep_to):
        mine = aux_buf.at[here]
        return remote(mine, mine, aux_send, aux_recv.at[side], ep_to, tp)

    def z_rows(z):
        return remote(
            rows_buf.at[0, here],
            rows_buf.at[0, here],
            rows_send,
            rows_recv.at[0, here],
            z * 2 + my_y,
            tp,
        )

    for z in far_first:
        z_rows(z).start()
    over_y = my_z * 2 + 1 - my_y
    rows_copy(0, here, over_y, tp, 0).start()
    rows_copy(2, here, over_y, tp, 2).start()

    total = nz * seqs
    sides = (my_y, 1 - my_y)

    def at_of(side, z):
        return sides[side] * nz + z

    def arrived(k, at):
        rows_copy(k, at, me, beside, k).wait_recv()

    there = at_of(1, my_z)
    def gather_z(z):
        at = at_of(0, z)
        arrived(0, at)
        rows_copy(0, at, over_y, tp, 0).start()
        rows_copy(0, at, me, across, 2).start()
        rows_copy(0, at, me, beside, 1, 0).start()

    for z in others[:-1]:
        gather_z(z)
    logits = lax.dot_general(
        feed, router_buf[...].astype(bf16), nt, preferred_element_type=f32
    )
    lane = lax.broadcasted_iota(jnp.int32, logits.shape, 1)
    same = lax.broadcasted_iota(jnp.int32, (seqs, seqs), 0) == lax.broadcasted_iota(
        jnp.int32, (seqs, seqs), 1
    )
    route = lax.dot_general(
        jnp.where(same, 1.0, 0.0).astype(bf16),
        route_ref[...].astype(f32).astype(bf16),
        nt,
        preferred_element_type=f32,
    ).astype(jnp.int32)
    picked = lane == route[:, 0:1]
    for k in range(1, route.shape[1]):
        picked = picked | (lane == route[:, k : k + 1])
    weights = jnp.exp(logits)
    pick = jnp.where(picked, weights, 0.0)
    group_lane = (lane - group_base) * group_size
    in_groups = (lane >= group_base) & (lane < group_base + group_count)
    group = jnp.where(in_groups, weights, 0.0)
    lead = route[:, 0:1]
    chosen = in_groups & (lead >= group_lane) & (lead < group_lane + group_size)
    group_weight = jnp.sum(jnp.where(chosen, weights, 0.0), axis=1, keepdims=True) / jnp.sum(
        group, axis=1, keepdims=True
    )
    pick = pick / jnp.sum(pick, axis=1, keepdims=True) * group_weight
    aux_buf[here] = jnp.where(lane == switch_lane, jax.nn.sigmoid(logits), pick).astype(bf16)
    for z in far_first:
        aux_copy(0, z * 2 + my_y).start()
    for z in far_first + [my_z]:
        aux_copy(1, z * 2 + 1 - my_y).start()
    gather_z(others[-1])
    arrived(0, there)
    rows_copy(0, there, me, beside, 1, 1).start()
    arrived(2, there)
    rows_copy(2, there, me, beside, 3, 1).start()
    for z in others:
        at = at_of(1, z)
        arrived(0, at)
        rows_copy(0, at, me, across, 2).start()
        rows_copy(0, at, me, beside, 1, 1).start()
    for z in others:
        at = at_of(0, z)
        arrived(2, at)
        rows_copy(2, at, me, beside, 3, 0).start()

    def gather_end(side):
        count = nz if side else nz - 1
        aux = aux_buf.at[0:count]
        remote(aux, aux, aux_send, aux_recv.at[side], me, beside).wait_recv()
        blocks = rows_buf.at[0:2, 0:count]
        remote(blocks, blocks, rows_send, side_recv.at[side], me, beside).wait_recv()

    def add(total_sum, value):
        return value if total_sum is None else total_sum + value

    def part_copy(k, side):
        block = pl.ds(sides[side] * nz, nz)
        return remote(
            part_buf.at[(diagonal, beside)[k], block],
            part_peer.at[k, block],
            part_send,
            part_recv.at[k, side],
            me,
            beside,
        )

    def feed_forward(side):
        block = pl.ds(sides[side] * nz, nz)
        gate = up = dense = None
        for k, q in enumerate(quarters):
            rows = rows_buf[k, block].reshape(total, quarter)
            span = pl.ds(pl.multiple_of(q * quarter, quarter), quarter)
            gate = add(gate, jnp.dot(rows, gate_w[span, :], preferred_element_type=f32))
            up = add(up, jnp.dot(rows, up_w[span, :], preferred_element_type=f32))
            pair = dense_w[pl.ds(q * 2, 2)].reshape(2 * share, quarter)
            dense = add(dense, lax.dot_general(rows, pair, nt, preferred_element_type=f32))
        dense_g, dense_u = dense[:, :share], dense[:, share:]
        aux = aux_buf[block].reshape(total, aux_buf.shape[2]).astype(f32)
        aux_lane = lax.broadcasted_iota(jnp.int32, aux.shape, 1)
        weight = jnp.sum(jnp.where(aux_lane == me, aux, 0.0), axis=1, keepdims=True)
        switch = jnp.sum(jnp.where(aux_lane == switch_lane, aux, 0.0), axis=1, keepdims=True)
        hidden = (gate * jax.nn.sigmoid(gate) * up * weight).astype(bf16)
        dense_hidden = (dense_g * jax.nn.sigmoid(dense_g) * dense_u * switch).astype(bf16)
        for k, q in enumerate((diagonal, beside, across, tp)):
            value = jnp.dot(hidden, down_w[q], preferred_element_type=f32) + jnp.dot(
                dense_hidden, dense_w[q + 8], preferred_element_type=f32
            )
            part_buf[q, block] = value.astype(bf16).reshape(nz, seqs, quarter)
            if k < 2:
                part_copy(k, side).start()

    far_then_own = far_first + [my_z]

    def x_copy(at):
        return remote(send_x.at[at], recv_x.at[at], x_send, x_recv.at[at], me, across)

    def sums_over_x(side):
        part_copy(0, side).wait_recv()
        for z in far_then_own:
            at = at_of(side, z)
            send_x[at] = (
                part_buf[across, at].astype(f32) + part_peer[0, at].astype(f32)
            ).astype(bf16)
            x_copy(at).start()

    def ep_copy(at, slot, ep_to):
        return remote(
            send_ep.at[at], recv_ep.at[slot], ep_send, ep_recv, ep_to, tp
        )

    def summed(at):
        x_copy(at).wait_recv()
        return (
            part_buf[tp, at].astype(f32)
            + part_peer[1, at].astype(f32)
            + recv_x[at].astype(f32)
        )

    def sums_over_ep(side):
        part_copy(1, side).wait_recv()
        for z in far_then_own if side else far_first:
            at = at_of(side, z)
            send_ep[at] = summed(at).astype(bf16)
            ep_copy(at, here, z * 2 + sides[side]).start()

    loaded(gate_w, 5)
    loaded(up_w, 6)
    loaded(down_w, 7)
    loaded(dense_w.at[0:3], 8)
    others_dense = dense_w.at[0:9]
    all_dense = remote(others_dense, others_dense, dense_send, dense_recv, me, beside)
    all_dense.wait_recv()
    gather_end(0)
    feed_forward(0)
    for z in others:
        at = at_of(1, z)
        arrived(2, at)
        rows_copy(2, at, me, beside, 3, 1).start()
    sums_over_x(0)
    gather_end(1)
    feed_forward(1)
    sums_over_x(1)
    sums_over_ep(0)
    combined = summed(here)
    sums_over_ep(1)

    seven = pl.ds(0, ep - 1)
    remote(send_ep.at[seven], recv_ep.at[seven], ep_send, ep_recv, me, beside).wait_recv()
    for side in range(2):
        for z in range(nz) if side else others:
            combined = combined + recv_ep[at_of(side, z)].astype(f32)

    square = jnp.sum(combined * combined, axis=1, keepdims=True)
    lanes = square_own.shape[1]
    row_id = lax.broadcasted_iota(jnp.int32, (seqs, lanes), 0)
    diagonal_lane = row_id == lax.broadcasted_iota(jnp.int32, (seqs, lanes), 1)
    square_row = jnp.sum(jnp.where(diagonal_lane, square, 0.0), axis=0, keepdims=True)
    square_own[...] = jnp.broadcast_to(square_row, square_own.shape)
    for k, peer in enumerate(near):
        remote(square_own, square_peer.at[k], square_send, square_recv, me, peer).start()
    all_squares = remote(square_peer, square_peer, square_send, square_recv, me, beside)
    all_squares.wait_recv()
    everything = (square_own[...] + square_peer[0]) + (square_peer[1] + square_peer[2])
    spread = jnp.where(diagonal_lane, everything[0:1], 0.0)
    scale = lax.rsqrt(jnp.sum(spread, axis=1, keepdims=True) / width + norm_eps)
    own_stream = stream_buf[tp].astype(f32)
    out_ref[...] = (own_stream + combined * scale * row(out_gain_ref)).astype(bf16)
    for copy in sends:
        copy.wait_send()
    blocks = rows_buf.at[:, seven]
    for ref, sem in (
        (blocks, rows_send),
        (aux_buf.at[seven], aux_send),
        (part_peer, part_send),
        (send_x, x_send),
        (send_ep.at[seven], ep_send),
    ):
        remote(ref, ref, sem, mix_recv.at[0], me, beside).wait_send()
    all_dense.wait_send()

    @pl.when(core == 1)
    def _():
        halves = rows_buf.at[0:2, 0:4]
        remote(halves, halves, mix_send.at[1], mix_recv.at[0], me, beside).wait_send()

    all_squares.wait_send()


def write_kernel(out_ref, state_ref, conv_ref, out_hbm, state_hbm, conv_hbm, sems):
    pairs = ((state_ref, state_hbm), (conv_ref, conv_hbm), (out_ref, out_hbm))
    copies = [pltpu.make_async_copy(src, dst, sems.at[k]) for k, (src, dst) in enumerate(pairs)]
    for copy in copies:
        copy.start()
    for copy in copies:
        copy.wait()


def fused_layer(
    resid,
    mix_gain,
    proj_x,
    proj_z,
    proj_b,
    proj_c,
    proj_step,
    step_bias,
    decay_rate,
    conv_taps,
    conv_state,
    scan_state,
    inner_gain,
    proj_out,
    post_gain,
    ffn_gain,
    group_router,
    expert_router,
    route_experts,
    expert_gate,
    expert_up,
    expert_down,
    dense_switch,
    dense_gate,
    dense_up,
    dense_down,
    out_gain,
):
    ep = lax.axis_size("ep")
    seqs, width = resid.shape
    quarter = width // 4
    channels = conv_state.shape[3]
    expert_count = expert_router.shape[1]
    group_count = group_router.shape[1]
    lanes = 128
    hidden_here = expert_gate.shape[2]
    share = dense_gate.shape[0] // 4
    bf16 = jnp.bfloat16
    vmem = pl.BlockSpec(memory_space=pltpu.VMEM)
    hbm = pl.BlockSpec(memory_space=pl.ANY)
    dma = pltpu.SemaphoreType.DMA
    kernel = functools.partial(
        fused_kernel, ep, expert_count // group_count, group_count, expert_count
    )
    earlier = conv_state.transpose(1, 2, 0, 3)
    state = scan_state.reshape(seqs, channels, scan_state.shape[3])
    results = pl.pallas_call(
        kernel,
        out_shape=(
            pltpu.VMEM((seqs, quarter), bf16),
            pltpu.VMEM(state.shape, state.dtype),
            pltpu.VMEM(earlier.shape, earlier.dtype),
        ),
        in_specs=[hbm] * 27,
        out_specs=(vmem, vmem, vmem),
        scratch_shapes=[
            pltpu.VMEM((4,) + proj_x.shape, bf16),
            pltpu.VMEM(state.shape, state.dtype),
            pltpu.VMEM((step_bias.shape[0], seqs, channels), jnp.float32),
            pltpu.VMEM((seqs, channels), jnp.float32),
            pltpu.VMEM((lanes, width), jnp.float32),
            pltpu.VMEM((width, hidden_here), bf16),
            pltpu.VMEM((width, hidden_here), bf16),
            pltpu.VMEM((4, hidden_here, quarter), bf16),
            pltpu.VMEM((12, share, quarter), bf16),
            pltpu.VMEM((4, seqs, quarter), bf16),
            pltpu.VMEM((seqs, width), bf16),
            pltpu.VMEM((seqs, width), bf16),
            pltpu.VMEM((2, seqs, width // 2), bf16),
            pltpu.VMEM((2, seqs, width // 2), bf16),
            pltpu.VMEM((4, ep, seqs, quarter), bf16),
            pltpu.VMEM((ep, seqs, lanes), bf16),
            pltpu.VMEM((4, ep, seqs, quarter), bf16),
            pltpu.VMEM((2, ep, seqs, quarter), bf16),
            pltpu.VMEM((ep, seqs, quarter), bf16),
            pltpu.VMEM((ep, seqs, quarter), bf16),
            pltpu.VMEM((ep, seqs, quarter), bf16),
            pltpu.VMEM((ep, seqs, quarter), bf16),
            pltpu.VMEM((8, lanes), jnp.float32),
            pltpu.VMEM((3, 8, lanes), jnp.float32),
            dma((9,)),
            dma,
            dma,
            dma((2,)),
            dma((3,)),
            dma,
            dma((2, ep)),
            dma,
            dma((2,)),
            dma,
            dma((2, 2)),
            dma,
            dma((ep,)),
            dma,
            dma,
            dma,
            dma,
            pltpu.SemaphoreType.REGULAR,
            dma((2,)),
            dma((16,)),
            pltpu.VMEM(proj_out.shape, proj_out.dtype),
            pltpu.VMEM(resid.shape, resid.dtype),
            pltpu.VMEM(mix_gain.shape, mix_gain.dtype),
            pltpu.VMEM(post_gain.shape, post_gain.dtype),
            pltpu.VMEM(ffn_gain.shape, ffn_gain.dtype),
            pltpu.VMEM(expert_router.T.shape, expert_router.T.dtype),
            pltpu.VMEM(group_router.T.shape, group_router.T.dtype),
            pltpu.VMEM(dense_switch.shape, dense_switch.dtype),
            pltpu.VMEM(route_experts.T.shape, route_experts.T.dtype),
            pltpu.VMEM(out_gain.shape, out_gain.dtype),
            pltpu.VMEM(inner_gain.shape, inner_gain.dtype),
            pltpu.VMEM(proj_step.T.shape, proj_step.T.dtype),
            pltpu.VMEM(conv_taps.shape, conv_taps.dtype),
            pltpu.VMEM(earlier.shape, earlier.dtype),
            pltpu.SMEM(step_bias.shape, step_bias.dtype),
            pltpu.SMEM(decay_rate.shape, decay_rate.dtype),
        ],
        compiler_params=pltpu.CompilerParams(collective_id=0, has_side_effects=True),
        name="fused_layer",
    )(
        proj_out,
        resid,
        mix_gain,
        post_gain,
        ffn_gain,
        expert_router.T,
        group_router.T,
        dense_switch,
        route_experts.T,
        out_gain,
        inner_gain,
        proj_step.T,
        conv_taps,
        earlier,
        step_bias,
        decay_rate,
        proj_x,
        proj_z,
        proj_b,
        proj_c,
        state,
        expert_gate,
        expert_up,
        expert_down,
        dense_gate,
        dense_up,
        dense_down,
    )
    layer_out, new_state, new_conv = pl.pallas_call(
        write_kernel,
        out_shape=tuple(jax.ShapeDtypeStruct(one.shape, one.dtype) for one in results),
        in_specs=[vmem] * 3,
        out_specs=(hbm, hbm, hbm),
        scratch_shapes=[dma((3,))],
        compiler_params=pltpu.CompilerParams(vmem_limit_bytes=4 << 20),
        name="write_results",
    )(*results)
    return layer_out, new_state.reshape(scan_state.shape), new_conv.transpose(2, 0, 1, 3)


def on_device(
    resid,
    mix_gain,
    proj_x,
    proj_z,
    proj_b,
    proj_c,
    proj_step,
    step_bias,
    decay_rate,
    conv_taps,
    conv_state,
    scan_state,
    inner_gain,
    proj_out,
    post_gain,
    ffn_gain,
    group_router,
    expert_router,
    route_experts,
    expert_gate,
    expert_up,
    expert_down,
    dense_switch,
    dense_gate,
    dense_up,
    dense_down,
    out_gain,
):
    tp_index = lax.axis_index("tp")
    seqs = resid.shape[0]
    width = resid.shape[1]
    quarter = width // lax.axis_size("tp")
    heads_here = scan_state.shape[1]
    head_dim = scan_state.shape[2]
    state_dim = scan_state.shape[3]
    channels = conv_state.shape[3]
    repeat = heads_here // (channels // state_dim)
    whole_blocks = 2 * seqs * route_experts.shape[1] // expert_router.shape[1] >= seqs
    one_group = channels == state_dim == 128 and expert_router.shape[1] <= 64
    few = lax.axis_size("tp") == 4 and expert_gate.shape[0] == 1
    few = few and lax.axis_size("ep") % 2 == 0
    if whole_blocks and one_group and few:
        return fused_layer(
            resid,
            mix_gain,
            proj_x,
            proj_z,
            proj_b,
            proj_c,
            proj_step,
            step_bias,
            decay_rate,
            conv_taps,
            conv_state,
            scan_state,
            inner_gain,
            proj_out,
            post_gain,
            ffn_gain,
            group_router,
            expert_router,
            route_experts,
            expert_gate,
            expert_up,
            expert_down,
            dense_switch,
            dense_gate,
            dense_up,
            dense_down,
            out_gain,
        )
    normed = scaled_rows(resid, mix_gain).astype(jnp.bfloat16)
    fresh = jnp.stack(
        [
            jnp.dot(normed, proj_x, preferred_element_type=jnp.float32),
            jnp.dot(normed, proj_b, preferred_element_type=jnp.float32),
            jnp.dot(normed, proj_c, preferred_element_type=jnp.float32),
        ],
        axis=1,
    ).astype(jnp.bfloat16)
    gate_z = jnp.dot(normed, proj_z, preferred_element_type=jnp.float32)
    step_all = jnp.dot(normed, proj_step, preferred_element_type=jnp.float32)
    step_raw = lax.dynamic_slice_in_dim(step_all, tp_index * heads_here, heads_here, 1)
    history = jnp.concatenate([conv_state, fresh[:, :, None, :]], axis=2)
    activated = jax.nn.silu(
        jnp.sum(history.astype(jnp.float32) * conv_taps.astype(jnp.float32)[None], axis=2)
    )
    xs_heads = activated[:, 0].reshape(seqs, heads_here, head_dim)
    b_heads = jnp.repeat(activated[:, 1].reshape(seqs, -1, state_dim), repeat, axis=1)
    c_heads = jnp.repeat(activated[:, 2].reshape(seqs, -1, state_dim), repeat, axis=1)
    step = jax.nn.softplus(step_raw + step_bias)
    keep = jnp.exp(-decay_rate * step)
    driven = step[:, :, None] * xs_heads
    new_state = keep[:, :, None, None] * scan_state + driven[:, :, :, None] * b_heads[:, :, None, :]
    read = jnp.sum(new_state * c_heads[:, :, None, :], axis=3).reshape(seqs, channels)
    gated = (read * jax.nn.silu(gate_z) * inner_gain.astype(jnp.float32)).astype(jnp.bfloat16)
    new_conv = history[:, :, 1:, :]
    mixed = lax.psum(
        jnp.dot(gated, proj_out, preferred_element_type=jnp.float32).astype(jnp.bfloat16), "tp"
    ).astype(jnp.float32)
    stream = (resid.astype(jnp.float32) + scaled_rows(mixed, post_gain)).astype(jnp.bfloat16)
    feed = scaled_rows(stream, ffn_gain).astype(jnp.bfloat16)
    feed_quarter = lax.dynamic_slice_in_dim(feed, tp_index * quarter, quarter, 1)
    expert_count = expert_router.shape[1]
    group_size = expert_count // group_router.shape[1]
    pick_count = route_experts.shape[1]
    group_prob = softmax_plain(jnp.dot(feed, group_router, preferred_element_type=jnp.float32))
    expert_logits = jnp.dot(feed, expert_router, preferred_element_type=jnp.float32)
    matches = route_experts[:, :, None] == jnp.arange(expert_count, dtype=jnp.int32)[None, None, :]
    pick_logits = jnp.sum(jnp.where(matches, expert_logits[:, None, :], 0.0), axis=2)
    chosen_group = route_experts[:, 0] // group_size
    group_ids = jnp.arange(group_router.shape[1], dtype=jnp.int32)
    group_weight = jnp.sum(
        jnp.where(chosen_group[:, None] == group_ids[None, :], group_prob, 0.0), axis=1
    )
    pick_weight = softmax_plain(pick_logits) * group_weight[:, None]
    capacity = 2 * seqs * pick_count // expert_count
    flat_picks = route_experts.reshape(-1)
    one_hot = (flat_picks[:, None] == jnp.arange(expert_count, dtype=jnp.int32)[None, :]).astype(
        jnp.int32
    )
    slot = jnp.sum((jnp.cumsum(one_hot, axis=0) - one_hot) * one_hot, axis=1)
    target = flat_picks * capacity + slot
    repeated = jnp.repeat(feed, pick_count, axis=0)
    outgoing = jnp.zeros((expert_count * capacity, width), jnp.bfloat16).at[target].set(repeated)
    outgoing = outgoing.reshape(expert_count, capacity, width)
    arrived = lax.all_to_all(outgoing, "ep", split_axis=0, concat_axis=0, tiled=True)
    sources = arrived.shape[0]
    items = arrived.shape[1]
    rows = arrived.reshape(sources * items, width)
    gate_value = jnp.dot(rows, expert_gate[0], preferred_element_type=jnp.float32)
    up_value = jnp.dot(rows, expert_up[0], preferred_element_type=jnp.float32)
    hidden = (jax.nn.silu(gate_value) * up_value).astype(jnp.bfloat16)
    result = jnp.dot(hidden, expert_down[0], preferred_element_type=jnp.float32).reshape(
        sources, items, width
    )
    summed = lax.psum_scatter(result.astype(jnp.bfloat16), "tp", scatter_dimension=2, tiled=True)
    returned = lax.all_to_all(summed, "ep", split_axis=0, concat_axis=0, tiled=True)
    fetched = returned.reshape(expert_count * capacity, quarter)[target].reshape(
        seqs, pick_count, quarter
    )
    routed = jnp.sum(fetched.astype(jnp.float32) * pick_weight[:, :, None], axis=1)
    gate_piece = jnp.einsum(
        "sd,cd->sc",
        feed_quarter,
        lax.all_gather(dense_gate, "ep", axis=0, tiled=True),
        preferred_element_type=jnp.float32,
    )
    up_piece = jnp.einsum(
        "sd,cd->sc",
        feed_quarter,
        lax.all_gather(dense_up, "ep", axis=0, tiled=True),
        preferred_element_type=jnp.float32,
    )
    gate_sum = gate_piece
    up_sum = up_piece
    gate_sum, up_sum = (
        lax.psum(gate_sum.astype(jnp.bfloat16), "tp").astype(jnp.float32),
        lax.psum(up_sum.astype(jnp.bfloat16), "tp").astype(jnp.float32),
    )
    dense_hidden = (jax.nn.silu(gate_sum) * up_sum).astype(jnp.bfloat16)
    dense_out = jnp.dot(
        dense_hidden,
        lax.all_gather(dense_down, "ep", axis=0, tiled=True),
        preferred_element_type=jnp.float32,
    )
    switch = jax.nn.sigmoid(jnp.dot(feed, dense_switch, preferred_element_type=jnp.float32))
    combined = routed + switch[:, None] * dense_out
    total_square = lax.psum(jnp.sum(combined * combined, axis=1), "tp")
    scale = lax.rsqrt(total_square / width + norm_eps)
    stream_part = lax.dynamic_slice_in_dim(stream, tp_index * quarter, quarter, 1).astype(
        jnp.float32
    )
    layer_out = (stream_part + combined * scale[:, None] * out_gain.astype(jnp.float32)).astype(
        jnp.bfloat16
    )
    return (layer_out, new_state, new_conv)


def solution(mesh):
    placed = (
        P("ep", None),
        P(),
        P(None, "tp"),
        P(None, "tp"),
        P(None, "tp"),
        P(None, "tp"),
        P(),
        P("tp"),
        P("tp"),
        P(None, None, "tp"),
        P("ep", None, None, "tp"),
        P("ep", "tp", None, None),
        P("tp"),
        P("tp", None),
        P(),
        P(),
        P(),
        P(),
        P("ep", None),
        P("ep", None, "tp"),
        P("ep", None, "tp"),
        P("ep", "tp", None),
        P(),
        P("ep", "tp"),
        P("ep", "tp"),
        P("ep", "tp"),
        P("tp"),
    )
    return jax.shard_map(
        on_device,
        mesh=mesh,
        in_specs=placed,
        out_specs=(P("ep", "tp"), P("ep", "tp", None, None), P("ep", None, None, "tp")),
        check_vma=False,
    )
```
